512 devices in a mesh: sp: 128 (over z, x, core), tp: 4 (over y).
Axes of the slice: x: 4, y: 4, z: 16, core: 2. Of those that a mesh axis runs over, the one named last changes fastest.
Arguments:
- tokens: bfloat16 [65536, 2048], P(('sp', 'tp')), may hold values from -8 to 8
- in_gain: float32 [2048], replicated, may hold values from 0.1 to 1.9
- w_conv_val: bfloat16 [2048, 1024], P('sp', 'tp'), may hold values from -0.125 to 0.125
- w_conv_gate: bfloat16 [2048, 1024], P('sp', 'tp'), may hold values from -0.125 to 0.125
- w_query: bfloat16 [2048, 1024], P('sp', 'tp'), may hold values from -1 to 1
- w_key: bfloat16 [2048, 256], P('sp', 'tp'), may hold values from -1 to 1
- value_weight: bfloat16 [2048, 256], P('sp', 'tp'), may hold values from -0.125 to 0.125
- conv_taps: float32 [31, 1024], P(None, 'tp'), may hold values from -1 to 1
- conv_bias: float32 [1024], P('tp'), may hold values from -3 to 3
- norm_gain: float32 [1024], P('tp'), may hold values from 0.1 to 1.9
- norm_bias: float32 [1024], P('tp'), may hold values from -3 to 3
- head_sink_logit: float32 [16], P('tp'), may hold values from 4 to 7
- w_out_conv: bfloat16 [1024, 2048], P('tp', 'sp'), may hold values from -0.125 to 0.125
- w_out_attn: bfloat16 [1024, 2048], P('tp', 'sp'), may hold values from -0.125 to 0.125
Outputs:
- mixed: bfloat16 [65536, 2048], P(('sp', 'tp'))
- log_total: float32 [65536, 16], P('sp', 'tp')
The draws below stay inside these ranges and needn't reach their ends.
All inputs are finite; a program needn't handle non-finite values.
Results may differ from the reference program's by a relative error of at most 0.012.
Values may be sent and summed in bfloat16 or wider, within the bound.
A program may use at most 64 MiB of HBM per device.

```python
import math
import jax
import jax.numpy as jnp
from jax import lax

MODEL_WIDTH = 2048
CONV = 1024
QUERY_HEADS = 16
KEY_VALUE_HEADS = 4
HEAD_WIDTH = 64
CONV_TAPS = 31
WINDOW_REACH = 128
TOK_DEV = 512
TOKENS = 65536


def planted_parts(key):
    random_seed_key = jax.random.fold_in(key, 101)
    direction = jnp.where(jax.random.bernoulli(jax.random.fold_in(random_seed_key, 1), 0.5, (MODEL_WIDTH,)), 1.0, -1.0).astype(jnp.float32)
    mask_pattern = jnp.where(jax.random.bernoulli(jax.random.fold_in(random_seed_key, 2), 0.5, (KEY_VALUE_HEADS, HEAD_WIDTH)), 1.0, -1.0).astype(jnp.float32)
    strength = math.sqrt(288.0) / HEAD_WIDTH ** 0.25
    return (direction, mask_pattern, strength)


def draw_tokens(key, part):
    direction, mask_pattern, strength = planted_parts(key)
    jitter = jnp.clip(jax.random.normal(jax.random.fold_in(key, 201), (TOKENS, MODEL_WIDTH), jnp.float32), -4.0, 4.0)
    levels = jnp.exp(jax.random.uniform(jax.random.fold_in(key, 202), (TOKENS, 1), jnp.float32, math.log(0.7), math.log(4.0)))
    chosen = jax.random.bernoulli(jax.random.fold_in(key, 203), 0.125, (TOKENS, 1))
    result = jnp.where(chosen, levels * direction[None, :] + jitter, jitter)
    return result.astype(jnp.bfloat16)


def draw_w_query(key, part):
    direction, mask_pattern, strength = planted_parts(key)
    random_draws = jnp.clip(jax.random.normal(jax.random.fold_in(key, 301), (MODEL_WIDTH, QUERY_HEADS * HEAD_WIDTH), jnp.float32), -4.0, 4.0) * MODEL_WIDTH ** (-0.5)
    column_list = jnp.repeat(mask_pattern, QUERY_HEADS // KEY_VALUE_HEADS, axis=0).reshape(QUERY_HEADS * HEAD_WIDTH)
    result = random_draws + strength / MODEL_WIDTH * direction[:, None] * column_list[None, :]
    return result.astype(jnp.bfloat16)


def draw_w_key(key, part):
    direction, mask_pattern, strength = planted_parts(key)
    random_draws = jnp.clip(jax.random.normal(jax.random.fold_in(key, 401), (MODEL_WIDTH, KEY_VALUE_HEADS * HEAD_WIDTH), jnp.float32), -4.0, 4.0) * MODEL_WIDTH ** (-0.5)
    column_list = mask_pattern.reshape(KEY_VALUE_HEADS * HEAD_WIDTH)
    result = random_draws + strength / MODEL_WIDTH * direction[:, None] * column_list[None, :]
    return result.astype(jnp.bfloat16)


def shard_levels(own_key, dims, split, smallest, high):
    def one(dim, parts):
        steps = jax.random.uniform(jax.random.fold_in(jax.random.fold_in(own_key, 6), dim), (parts,), jnp.float32, smallest / len(split), high / len(split))
        return jnp.repeat(jnp.exp(steps), dims[dim] // parts).reshape((-1,) + (1,) * (len(dims) - dim - 1))

    factor_of = one(*split[0])
    for cut in split[1:]:
        factor_of = factor_of * one(*cut)
    return factor_of


def centred(key, extent, scale, most, shards=(), held_as=jnp.bfloat16):
    entries = scale * jax.random.normal(key, extent, jnp.float32)
    if shards:
        entries = entries * shard_levels(key, extent, shards, -0.22, 0.18)
    return jnp.clip(entries, -most, most).astype(held_as)


def setup_inputs(seed: int = 0) -> dict:
    splits = jax.random.split(jax.random.key(seed), 15)
    return {
        "tokens": draw_tokens(jax.random.fold_in(splits[14], 71), 0),
        "in_gain": jnp.clip(1.0 + 0.18 * jax.random.normal(splits[1], (MODEL_WIDTH,), jnp.float32), 0.1, 1.9),
        "w_conv_val": centred(splits[2], (MODEL_WIDTH, CONV), MODEL_WIDTH ** -0.5, 0.125, ((0, 128), (1, 4))),
        "w_conv_gate": centred(splits[3], (MODEL_WIDTH, CONV), MODEL_WIDTH ** -0.5, 0.125, ((0, 128), (1, 4))),
        "w_query": draw_w_query(jax.random.fold_in(splits[14], 71), 0),
        "w_key": draw_w_key(jax.random.fold_in(splits[14], 71), 0),
        "value_weight": centred(splits[6], (MODEL_WIDTH, KEY_VALUE_HEADS * HEAD_WIDTH), MODEL_WIDTH ** -0.5, 0.125, ((0, 128), (1, 4))),
        "conv_taps": centred(splits[7], (CONV_TAPS, CONV), CONV_TAPS ** -0.5, 1.0, ((1, 4),), jnp.float32),
        "conv_bias": centred(splits[8], (CONV,), 0.5, 3.0, ((0, 4),), jnp.float32),
        "norm_gain": jnp.clip(1.0 + 0.18 * jax.random.normal(splits[9], (CONV,), jnp.float32), 0.1, 1.9),
        "norm_bias": centred(splits[10], (CONV,), 0.5, 3.0, ((0, 4),), jnp.float32),
        "head_sink_logit": jnp.clip(4.0 + 3.0 * jax.random.uniform(splits[11], (QUERY_HEADS,), jnp.float32) ** shard_levels(splits[11], (QUERY_HEADS,), ((0, 4),), -0.2, 0.2), 4.0, 7.0),
        "w_out_conv": centred(splits[12], (CONV, MODEL_WIDTH), (CONV + QUERY_HEADS * HEAD_WIDTH) ** -0.5, 0.125, ((0, 4), (1, 128))),
        "w_out_attn": centred(splits[13], (QUERY_HEADS * HEAD_WIDTH, MODEL_WIDTH), (CONV + QUERY_HEADS * HEAD_WIDTH) ** -0.5, 0.125, ((0, 4), (1, 128))),
    }


def reference(tokens, in_gain, w_conv_val, w_conv_gate, w_query, w_key, value_weight, conv_taps, conv_bias, norm_gain, norm_bias, head_sink_logit, w_out_conv, w_out_attn):
    every_row = tokens.shape[0]
    flt = tokens.astype(jnp.float32)
    normed = (flt * lax.rsqrt(lax.optimization_barrier(jnp.mean(flt * flt, axis=-1, keepdims=True)) + 1e-06) * in_gain).astype(jnp.bfloat16)
    val_part = jnp.dot(normed, w_conv_val, preferred_element_type=jnp.float32)
    gate_part = jnp.dot(normed, w_conv_gate, preferred_element_type=jnp.float32)
    glu = (val_part * jax.nn.sigmoid(gate_part)).astype(jnp.bfloat16)
    half = CONV_TAPS // 2
    padded = jnp.pad(glu, ((half, half), (0, 0)))
    filtered = jnp.zeros(glu.shape, jnp.float32) + conv_bias
    for offset in range(CONV_TAPS):
        filtered = filtered + padded[offset:offset + every_row].astype(jnp.float32) * conv_taps[offset]
    center = lax.optimization_barrier(jnp.mean(filtered, axis=-1, keepdims=True))
    spread = lax.optimization_barrier(jnp.mean((filtered - center) ** 2, axis=-1, keepdims=True))
    conv_out = jax.nn.silu((filtered - center) * lax.rsqrt(spread + 1e-05) * norm_gain + norm_bias).astype(jnp.bfloat16)
    query_matrix = jnp.dot(normed, w_query, preferred_element_type=jnp.float32).astype(jnp.bfloat16)
    key = jnp.dot(normed, w_key, preferred_element_type=jnp.float32).astype(jnp.bfloat16)
    value_matrix = jnp.dot(normed, value_weight, preferred_element_type=jnp.float32).astype(jnp.bfloat16)
    query_groups = QUERY_HEADS // KEY_VALUE_HEADS
    query4_grouped = query_matrix.reshape(every_row, KEY_VALUE_HEADS, query_groups, HEAD_WIDTH)
    padded_keys = jnp.pad(key.reshape(every_row, KEY_VALUE_HEADS, HEAD_WIDTH), ((WINDOW_REACH, WINDOW_REACH), (0, 0), (0, 0)))
    padded_values = jnp.pad(value_matrix.reshape(every_row, KEY_VALUE_HEADS, HEAD_WIDTH), ((WINDOW_REACH, WINDOW_REACH), (0, 0), (0, 0)))
    block = TOK_DEV
    sink_column = head_sink_logit.reshape(KEY_VALUE_HEADS, query_groups, 1)

    def attend(index):
        first = (index * block).astype(jnp.int32)
        qblock = lax.dynamic_slice_in_dim(query4_grouped, first, block, 0).astype(jnp.float32)
        kblock = lax.dynamic_slice_in_dim(padded_keys, first, block + 2 * WINDOW_REACH, 0).astype(jnp.float32)
        vblock = lax.dynamic_slice_in_dim(padded_values, first, block + 2 * WINDOW_REACH, 0).astype(jnp.float32)
        scores = jnp.einsum('qkgd,jkd->kgqj', qblock, kblock) * HEAD_WIDTH ** (-0.5)
        qpos = first + jnp.arange(block, dtype=jnp.int32)
        kpos = first - WINDOW_REACH + jnp.arange(block + 2 * WINDOW_REACH, dtype=jnp.int32)
        valid = (jnp.abs(qpos[:, None] - kpos[None, :]) <= WINDOW_REACH) & (kpos[None, :] >= 0) & (kpos[None, :] < every_row)
        masked = jnp.where(valid, scores, -1e+30)
        top = jnp.maximum(lax.optimization_barrier(jnp.max(masked, axis=-1)), sink_column)
        expd = jnp.where(valid, jnp.exp(masked - top[..., None]), 0.0)
        total = lax.optimization_barrier(jnp.sum(expd, axis=-1)) + jnp.exp(sink_column - top)
        probs = (expd / total[..., None]).astype(jnp.bfloat16)
        attended = jnp.einsum('kgqj,jkd->qkgd', probs.astype(jnp.float32), vblock).astype(jnp.bfloat16)
        log_block = (top + jnp.log(total)).reshape(QUERY_HEADS, block).T
        return (attended.reshape(block, QUERY_HEADS * HEAD_WIDTH), log_block)
    attended, log_total = lax.map(attend, jnp.arange(every_row // block, dtype=jnp.int32))
    attended = attended.reshape(every_row, QUERY_HEADS * HEAD_WIDTH)
    log_total = log_total.reshape(every_row, QUERY_HEADS)
    features = jnp.concatenate([conv_out, attended], axis=1)
    weights_all = jnp.concatenate([w_out_conv, w_out_attn], axis=0)
    mixed = jnp.dot(features, weights_all, preferred_element_type=jnp.float32).astype(jnp.bfloat16)
    return (mixed, log_total)
```

```python
import jax
import jax.numpy as jnp
from jax import lax
from jax.experimental import pallas as pl
from jax.experimental.pallas import tpu as pltpu
from jax.sharding import Mesh
from jax.sharding import PartitionSpec as P

MESH = pl.DeviceIdType.MESH
REACH = 128
HEADS = 4
HALF = 15
RING = 16
LAG_RELAY = 1
LAG_PAIR = 2
F32 = jnp.float32
BF16 = jnp.bfloat16
SP = ("z", "x", "c")
SP_TP = ("z", "x", "c", "y")


def nt_dot(a, b):
    return lax.dot_general(a, b, (((1,), (1,)), ((), ())), preferred_element_type=F32)


def layer(
    tok, gain, w_val, w_gate, w_q, w_k, w_v, w_oc, w_oa, taps, cbias, ngain, nbias, sink,
    mixed, log_out,
    wg, og, tg, glu_s, q_s, kv_s, kvw, padf, filt, stat, st_tx, st_rx, feat, mask_s,
    part, tx2, rx2, txp, rxp,
    r_wz, s_wz, r_wx, s_wx, r_wp, s_wp, r_ox, s_ox, r_oz, s_oz, r_op, s_op, r_t, s_t,
    r_h, s_h, r_st, s_st, r_r2, s_r2, r_rp, s_rp,
):
    z, x, c, y = (lax.axis_index(n) for n in ("z", "x", "c", "y"))
    d = 1 - 2 * c
    zp, zm = lax.rem(z + 1, 16), lax.rem(z + 15, 16)
    xr, xl = lax.rem(x + 4 + d, 4), lax.rem(x + 4 - d, 4)
    x2 = lax.rem(x + 2, 4)
    yp, ym, y2 = lax.rem(y + 1, 4), lax.rem(y + 3, 4), lax.rem(y + 2, 4)
    other = 1 - c
    me = z * 8 + x * 2 + c
    nxt, prv = lax.rem(me + 1, 128), lax.rem(me + 127, 128)

    def at_sp(s):
        return {"z": s // 8, "x": lax.rem(s // 2, 4), "c": lax.rem(s, 2)}

    def copy(src, dst, ssem, rsem, dev):
        return pltpu.make_async_remote_copy(
            src_ref=src, dst_ref=dst, send_sem=ssem, recv_sem=rsem,
            device_id=dev, device_id_type=MESH,
        )

    sent = []

    def send(src, dst, ssem, rsem, dev):
        cp = copy(src, dst, ssem, rsem, dev)
        cp.start()
        sent.append(cp)

    def got(dst, ssem, rsem, dev):
        copy(dst, dst, ssem, rsem, dev).wait_recv()

    barrier = pltpu.get_barrier_semaphore()
    greet = [{"z": zp}, {"z": zm}, {"x": xr}, {"x": xl}, {"c": other}, {"y": yp}, {"y": ym}, {"y": y2},
             at_sp(nxt), at_sp(prv)]
    for dev in greet:
        pl.semaphore_signal(barrier, inc=1, device_id=dev, device_id_type=MESH)

    wg[z, x, c] = jnp.concatenate([w_val[...], w_gate[...], w_q[...], w_k[...], w_v[...]], axis=1)
    eye = (
        lax.broadcasted_iota(jnp.int32, (16, 16), 0) == lax.broadcasted_iota(jnp.int32, (16, 16), 1)
    ).astype(BF16)
    og[z, x, c] = jnp.concatenate([nt_dot(eye, w_oc[...]), nt_dot(eye, w_oa[...])], axis=1).astype(BF16)
    t = tok[...].astype(F32)
    inv = lax.rsqrt(jnp.mean(t * t, axis=-1, keepdims=True) + 1e-06)
    normed = (t * inv * gain[...]).astype(BF16)
    tg[y, 0] = normed[:, :1024]
    tg[y, 1] = normed[:, 1024:]
    row = lax.broadcasted_iota(jnp.int32, (128, 384), 0)
    col = lax.broadcasted_iota(jnp.int32, (128, 384), 1)
    mask_s[...] = jnp.where((col >= row) & (col <= row + 2 * REACH), 0.0, -1e30).astype(F32)

    pl.semaphore_wait(barrier, len(greet))

    send(tg.at[y, 0], tg.at[y, 0], s_t.at[0], r_t.at[0], {"y": yp})
    send(tg.at[y, 1], tg.at[y, 1], s_t.at[1], r_t.at[1], {"y": ym})
    def wblk(zi, xi):
        return wg.at[zi, xi, c]

    def oblk(zi, h):
        return og.at[zi, 2 * h : 2 * h + 2, c]

    def plus(k):
        return lax.rem(z + 16 - k, 16)

    def minus(k):
        return lax.rem(z + k, 16)

    def w_forward(k, up):
        zi = plus(k) if up else minus(k)
        i = k if up else 8 + k
        send(wblk(zi, x), wblk(zi, x), s_wz.at[i], r_wz.at[i], {"z": zp if up else zm})

    def o_forward(k, up, h):
        zi = plus(k) if up else minus(k)
        i = 2 * (k if up else 8 + k) + h
        send(oblk(zi, h), oblk(zi, h), s_oz.at[i], r_oz.at[i], {"z": zp if up else zm})

    def w_sideways(zi, r):
        send(wblk(zi, x), wblk(zi, x), s_wx.at[r], r_wx.at[r], {"x": xr})
        send(wblk(zi, x), wblk(zi, x), s_wx.at[16 + r], r_wx.at[16 + r], {"x": xl})

    def members(k):
        out = []
        if 0 <= k <= 8:
            out.append((plus(k), k))
        if 1 <= k <= 7:
            out.append((minus(k), 8 + k))
        return out

    own_o = og.at[z, x, c]
    send(own_o, own_o, s_ox.at[0], r_ox.at[0], {"x": xr})
    send(own_o, own_o, s_ox.at[1], r_ox.at[1], {"x": xl})
    for k in range(0, 9 + LAG_PAIR):
        if k == 0:
            w_forward(0, True)
            w_forward(0, False)
        if 1 <= k <= 8:
            got(wblk(plus(k), x), s_wz.at[k - 1], r_wz.at[k - 1], {"z": zm})
            if k < 8:
                w_forward(k, True)
        if 1 <= k <= 7:
            got(wblk(minus(k), x), s_wz.at[8 + k - 1], r_wz.at[8 + k - 1], {"z": zp})
            if k < 7:
                w_forward(k, False)
        for zi, r in members(k):
            w_sideways(zi, r)
        if k == 0:
            send(tg.at[y, 1], tg.at[y, 1], s_t.at[2], r_t.at[2], {"y": yp})
            send(tg.at[y, 0], tg.at[y, 0], s_t.at[3], r_t.at[3], {"y": ym})
            from_l, from_r = og.at[z, xl, c], og.at[z, xr, c]
            got(from_l, s_ox.at[0], r_ox.at[0], {"x": xl})
            send(from_l, from_l, s_ox.at[2], r_ox.at[2], {"x": xr})
            got(from_r, s_ox.at[1], r_ox.at[1], {"x": xr})
            got(og.at[z, x2, c], s_ox.at[2], r_ox.at[2], {"x": xl})
            for h in range(2):
                o_forward(0, True, h)
                o_forward(0, False, h)
        for h in range(2):
            if 1 <= k <= 8:
                got(oblk(plus(k), h), s_oz.at[2 * (k - 1) + h], r_oz.at[2 * (k - 1) + h], {"z": zm})
                if k < 8:
                    o_forward(k, True, h)
            if 1 <= k <= 7:
                i = 2 * (8 + k - 1) + h
                got(oblk(minus(k), h), s_oz.at[i], r_oz.at[i], {"z": zp})
                if k < 7:
                    o_forward(k, False, h)
        for zi, r in members(k):
            send(og.at[zi, :, c], og.at[zi, :, c], s_op.at[r], r_op.at[r], {"c": other})
        for zi, r in members(k - LAG_RELAY):
            got(wblk(zi, xl), s_wx.at[r], r_wx.at[r], {"x": xl})
            send(wblk(zi, xl), wblk(zi, xl), s_wx.at[32 + r], r_wx.at[32 + r], {"x": xr})
        for zi, r in members(k - LAG_PAIR):
            got(wblk(zi, xr), s_wx.at[16 + r], r_wx.at[16 + r], {"x": xr})
            got(wblk(zi, x2), s_wx.at[32 + r], r_wx.at[32 + r], {"x": xl})
            send(wg.at[zi, :, c], wg.at[zi, :, c], s_wp.at[r], r_wp.at[r], {"c": other})
        if k == 3:
            got(tg.at[ym, 0], s_t.at[0], r_t.at[0], {"y": ym})
            send(tg.at[ym, 0], tg.at[ym, 0], s_t.at[4], r_t.at[4], {"y": yp})
            got(tg.at[yp, 1], s_t.at[1], r_t.at[1], {"y": yp})
            send(tg.at[yp, 1], tg.at[yp, 1], s_t.at[5], r_t.at[5], {"y": ym})
    for k in range(9):
        for zi, r in members(k):
            got(wg.at[zi, :, other], s_wp.at[r], r_wp.at[r], {"c": other})
    got(tg.at[ym, 1], s_t.at[2], r_t.at[2], {"y": ym})
    got(tg.at[yp, 0], s_t.at[3], r_t.at[3], {"y": yp})
    got(tg.at[y2, 0], s_t.at[4], r_t.at[4], {"y": ym})
    got(tg.at[y2, 1], s_t.at[5], r_t.at[5], {"y": yp})

    rows = 512
    ta = tg[:, 0].reshape(rows, 1024)
    tb = tg[:, 1].reshape(rows, 1024)

    def project(lo, hi):
        wa = wg[0:8, :, :, :, lo:hi].reshape(1024, hi - lo)
        wb = wg[8:16, :, :, :, lo:hi].reshape(1024, hi - lo)
        return jnp.dot(ta, wa, preferred_element_type=F32) + jnp.dot(tb, wb, preferred_element_type=F32)

    glu_s[16 : 16 + rows] = (project(0, 256) * jax.nn.sigmoid(project(256, 512))).astype(BF16)
    kv_s[REACH : REACH + rows] = project(768, 896).astype(BF16)
    send(glu_s.at[16:32], glu_s.at[528:544], s_h.at[0], r_h.at[0], at_sp(prv))
    send(glu_s.at[512:528], glu_s.at[0:16], s_h.at[1], r_h.at[1], at_sp(nxt))
    q_s[...] = (project(512, 768) * 0.125).astype(BF16)
    send(kv_s.at[128:256], kv_s.at[640:768], s_h.at[2], r_h.at[2], at_sp(prv))
    send(kv_s.at[512:640], kv_s.at[0:128], s_h.at[3], r_h.at[3], at_sp(nxt))

    got(glu_s.at[528:544], s_h.at[0], r_h.at[0], at_sp(nxt))
    got(glu_s.at[0:16], s_h.at[1], r_h.at[1], at_sp(prv))
    first = (me > 0).astype(F32)
    last = (me < 127).astype(F32)
    for l in range(2):
        lanes = slice(128 * l, 128 * l + 128)
        padf[l, 0:16] = glu_s[0:16, lanes].astype(F32) * first
        padf[l, 16:528] = glu_s[16:528, lanes].astype(F32)
        padf[l, 528:544] = glu_s[528:544, lanes].astype(F32) * last

    lane64 = lax.broadcasted_iota(jnp.int32, (64, 128), 1)

    def conv_rows(i, carry):
        r0 = i * 64
        accs = []
        for l in range(2):
            lanes = slice(128 * l, 128 * l + 128)
            acc = jnp.broadcast_to(cbias[0:1, lanes], (64, 128))
            for j in range(2 * HALF + 1):
                acc = acc + padf[l, pl.ds(r0 + j + 1, 64), :] * taps[j : j + 1, lanes]
            filt[pl.ds(r0, 64), lanes] = acc
            accs.append(acc)
        s1 = jnp.sum(accs[0] + accs[1], axis=1, keepdims=True)
        s2 = jnp.sum(accs[0] * accs[0] + accs[1] * accs[1], axis=1, keepdims=True)
        stat[pl.ds(r0, 64), :] = jnp.where(lane64 == 0, s1, jnp.where(lane64 == 1, s2, 0.0))
        return carry

    lax.fori_loop(0, 8, conv_rows, 0)
    st_tx[...] = jnp.transpose(stat[...])[0:8, :]

    got(kv_s.at[640:768], s_h.at[2], r_h.at[2], at_sp(nxt))
    got(kv_s.at[0:128], s_h.at[3], r_h.at[3], at_sp(prv))
    kvf = kv_s[...].astype(F32)
    turned = pltpu.roll(kvf, 64, 1)
    low = lax.broadcasted_iota(jnp.int32, (768, 128), 1) < 64
    kvw[0] = jnp.where(low, kvf, 0.0).astype(BF16)
    kvw[1] = jnp.where(low, 0.0, turned).astype(BF16)
    kvw[2] = jnp.where(low, turned, 0.0).astype(BF16)
    kvw[3] = jnp.where(low, 0.0, kvf).astype(BF16)

    for i, dev in enumerate((yp, ym, y2)):
        send(st_tx, st_rx.at[i], s_st.at[i], r_st.at[i], {"y": dev})

    low128 = lax.broadcasted_iota(jnp.int32, (128, 128), 1) < 64
    ends = lax.broadcasted_iota(jnp.int32, (1, 384), 1)

    def attend(i, carry):
        q0 = pl.multiple_of(i * 128, 128)
        pos = me * 512 + i * 128 - REACH + ends
        edge = jnp.where((pos >= 0) & (pos < 65536), 0.0, -1e30).astype(F32)
        bias = mask_s[...] + edge
        for p in range(2):
            qp = q_s[pl.ds(q0, 128), 128 * p : 128 * p + 128]
            probs, inverse = [], []
            for b in range(2):
                h = 2 * p + b
                s = nt_dot(qp, kvw[b, pl.ds(q0, 384), :]) + bias
                top = jnp.maximum(jnp.max(s, axis=1, keepdims=True), sink[h])
                e = jnp.exp(s - top)
                total = jnp.sum(e, axis=1, keepdims=True) + jnp.exp(sink[h] - top)
                log_out[pl.ds(q0, 128), h : h + 1] = top + jnp.log(total)
                probs.append(e.astype(BF16))
                inverse.append(1.0 / total)
            o = jnp.dot(probs[0], kvw[2, pl.ds(q0, 384), :], preferred_element_type=F32)
            o = o + jnp.dot(probs[1], kvw[3, pl.ds(q0, 384), :], preferred_element_type=F32)
            o = o * jnp.where(low128, inverse[0], inverse[1])
            feat[pl.ds(q0, 128), 256 + 128 * p : 384 + 128 * p] = o.astype(BF16)
        return carry

    lax.fori_loop(0, 4, attend, 0)

    for i, dev in enumerate((ym, yp, y2)):
        got(st_rx.at[i], s_st.at[i], r_st.at[i], {"y": dev})
    both = st_tx[...] + st_rx[0] + st_rx[1] + st_rx[2]
    stat[...] = jnp.transpose(jnp.concatenate([both, jnp.zeros((120, 512), F32)], axis=0)) * (1.0 / 1024.0)

    def norm_rows(i, carry):
        r0 = pl.multiple_of(i * 128, 128)
        mean = stat[pl.ds(r0, 128), 0:1]
        var = stat[pl.ds(r0, 128), 1:2] - mean * mean
        v = (filt[pl.ds(r0, 128), :] - mean) * lax.rsqrt(var + 1e-05) * ngain[...] + nbias[...]
        feat[pl.ds(r0, 128), 0:256] = (v * jax.nn.sigmoid(v)).astype(BF16)
        return carry

    lax.fori_loop(0, 4, norm_rows, 0)

    for k in range(9):
        for zi, r in members(k):
            got(og.at[zi, :, other], s_op.at[r], r_op.at[r], {"c": other})

    def out_half(block, half):
        f = feat[pl.ds(pl.multiple_of(block * 128, 128), 128), :]
        return nt_dot(f, og[8 * half : 8 * half + 8].reshape(1024, 512))

    tx2[0] = out_half(y2, 0).astype(BF16)
    tx2[1] = out_half(y2, 1).astype(BF16)
    send(tx2.at[0], rx2.at[0], s_r2.at[0], r_r2.at[0], {"y": yp})
    txp[0, 1] = out_half(yp, 1).astype(BF16)
    send(tx2.at[1], rx2.at[1], s_r2.at[1], r_r2.at[1], {"y": ym})
    txp[1, 0] = out_half(ym, 0).astype(BF16)
    send(txp.at[0, 1], rxp.at[0, 1], s_rp.at[1], r_rp.at[1], {"y": yp})
    part[0] = out_half(yp, 0)
    send(txp.at[1, 0], rxp.at[1, 0], s_rp.at[2], r_rp.at[2], {"y": ym})
    part[1] = out_half(ym, 1)
    part[2] = out_half(y, 0)
    part[3] = out_half(y, 1)
    got(rx2.at[0], s_r2.at[0], r_r2.at[0], {"y": ym})
    txp[0, 0] = (part[0] + rx2[0].astype(F32)).astype(BF16)
    got(rx2.at[1], s_r2.at[1], r_r2.at[1], {"y": yp})
    txp[1, 1] = (part[1] + rx2[1].astype(F32)).astype(BF16)
    send(txp.at[0, 0], rxp.at[0, 0], s_rp.at[0], r_rp.at[0], {"y": yp})
    send(txp.at[1, 1], rxp.at[1, 1], s_rp.at[3], r_rp.at[3], {"y": ym})
    for a, h in ((0, 1), (1, 0), (0, 0), (1, 1)):
        got(rxp.at[a, h], s_rp.at[2 * a + h], r_rp.at[2 * a + h], {"y": ym if a == 0 else yp})
    for h in range(2):
        total = part[2 + h] + rxp[0, h].astype(F32) + rxp[1, h].astype(F32)
        mixed[:, 1024 * h : 1024 * h + 1024] = total.astype(BF16)
    for cp in sent:
        cp.wait_send()


def on_device(
    tokens, in_gain, w_conv_val, w_conv_gate, w_query, w_key, value_weight, conv_taps, conv_bias,
    norm_gain, norm_bias, head_sink_logit, w_out_conv, w_out_attn,
):
    vm = pl.BlockSpec(memory_space=pltpu.VMEM)
    dma = pltpu.SemaphoreType.DMA
    scratch = [
        pltpu.VMEM((16, 4, 2, 16, 896), BF16),
        pltpu.VMEM((16, 4, 2, 16, 512), BF16),
        pltpu.VMEM((4, 2, 128, 1024), BF16),
        pltpu.VMEM((544, 256), BF16),
        pltpu.VMEM((512, 256), BF16),
        pltpu.VMEM((768, 128), BF16),
        pltpu.VMEM((4, 768, 128), BF16),
        pltpu.VMEM((2, 544, 128), F32),
        pltpu.VMEM((512, 256), F32),
        pltpu.VMEM((512, 128), F32),
        pltpu.VMEM((8, 512), F32),
        pltpu.VMEM((3, 8, 512), F32),
        pltpu.VMEM((512, 512), BF16),
        pltpu.VMEM((128, 384), F32),
        pltpu.VMEM((4, 128, 1024), F32),
        pltpu.VMEM((2, 128, 1024), BF16),
        pltpu.VMEM((2, 128, 1024), BF16),
        pltpu.VMEM((2, 2, 128, 1024), BF16),
        pltpu.VMEM((2, 2, 128, 1024), BF16),
    ]
    for n in (16, 48, 16, 3, 32, 16, 6, 4, 3, 2, 4):
        scratch += [dma((n,)), dma((n,))]
    return pl.pallas_call(
        layer,
        name="layer",
        out_shape=(
            jax.ShapeDtypeStruct((128, 2048), BF16),
            jax.ShapeDtypeStruct((512, 4), F32),
        ),
        in_specs=[vm] * 13 + [pl.BlockSpec(memory_space=pltpu.SMEM)],
        out_specs=(vm, vm),
        scratch_shapes=scratch,
        compiler_params=pltpu.CompilerParams(
            collective_id=0, has_side_effects=True, vmem_limit_bytes=56 * 1024 * 1024
        ),
    )(
        tokens, in_gain[None], w_conv_val, w_conv_gate, w_query, w_key, value_weight,
        w_out_conv, w_out_attn, conv_taps, conv_bias[None], norm_gain[None], norm_bias[None],
        head_sink_logit,
    )


def solution(mesh):
    finer = Mesh(mesh.devices.reshape(16, 4, 2, mesh.shape["tp"]), ("z", "x", "c", "y"))
    in_specs = (
        P(SP_TP, None), P(),
        P(SP, "y"), P(SP, "y"), P(SP, "y"), P(SP, "y"), P(SP, "y"),
        P(None, "y"), P("y"), P("y"), P("y"), P("y"),
        P("y", SP), P("y", SP),
    )
    return jax.shard_map(
        on_device, mesh=finer, in_specs=in_specs, out_specs=(P(SP_TP, None), P(SP, "y")), check_vma=False
    )
```

```python
import jax
import jax.numpy as jnp
from jax import lax
from jax.experimental import pallas as pl
from jax.experimental.pallas import tpu as pltpu
from jax.sharding import Mesh
from jax.sharding import PartitionSpec as P

MESH = pl.DeviceIdType.MESH
REACH = 128
HEADS = 4
HALF = 15
F32 = jnp.float32
BF16 = jnp.bfloat16
SP = ("z", "x", "c")
SP_TP = ("z", "x", "c", "y")


def nt_dot(a, b):
    return lax.dot_general(a, b, (((1,), (1,)), ((), ())), preferred_element_type=F32)


def layer(
    tok_h, gain_h, val_h, gate_h, wq_h, wk_h, wv_h, oc_h, oa_h, taps_h, cbias_h, ngain_h, nbias_h, sink,
    mixed, log_out,
    tok, gain, wk, wv, taps, cbias, ngain, nbias,
    wg, og, tg, glu_s, q_s, kv_s, kvw, padf, filt, stat, lstat, st_tx, st_rx, feat, mask_s,
    part, tx2, rx2, txp, rxp, s_in,
    r_wz, r_wx, r_wg, r_wp, r_ox, r_oz, r_on, r_op, r_t, r_h, r_st, r_r2, r_rp, out_sem,
):
    z, x, c, y = (lax.axis_index(n) for n in ("z", "x", "c", "y"))
    d = 1 - 2 * c

    def along(e):
        return lax.rem(z + 16 + e, 16)

    xr, xl = lax.rem(x + 4 + d, 4), lax.rem(x + 4 - d, 4)
    x2 = lax.rem(x + 2, 4)
    yp, ym, y2 = lax.rem(y + 1, 4), lax.rem(y + 3, 4), lax.rem(y + 2, 4)
    other = 1 - c
    me = z * 8 + x * 2 + c
    nxt, prv = lax.rem(me + 1, 128), lax.rem(me + 127, 128)

    def at_sp(s):
        return {"z": s // 8, "x": lax.rem(s // 2, 4), "c": lax.rem(s, 2)}

    def copy(src, dst, ssem, rsem, dev):
        return pltpu.make_async_remote_copy(
            src_ref=src, dst_ref=dst, send_sem=ssem, recv_sem=rsem,
            device_id=dev, device_id_type=MESH,
        )

    open_scope = []

    def phase(name):
        if open_scope:
            open_scope.pop().__exit__(None, None, None)
        if name:
            scope = jax.named_scope(name)
            scope.__enter__()
            open_scope.append(scope)

    def send(src, dst, ssem, rsem, dev):
        copy(src, dst, ssem, rsem, dev).start()

    def got(dst, ssem, rsem, dev):
        copy(dst, dst, ssem, rsem, dev).wait_recv()

    phase("greet")
    barrier = pltpu.get_barrier_semaphore()
    greet = [{"z": along(e)} for e in (1, -1, 2, -2, 4, -4, 8)]
    greet += [{"x": xr}, {"x": xl}, {"c": other}, {"y": yp}, {"y": ym}, {"y": y2}, at_sp(nxt), at_sp(prv)]
    for dev in greet:
        pl.semaphore_signal(barrier, inc=1, device_id=dev, device_id_type=MESH)

    wown, oown = wg.at[z, x, c], og.at[z, x, c]
    loads = [
        pltpu.make_async_copy(src, dst, s_in.at[i])
        for i, (src, dst) in enumerate((
            (tok_h, tok), (gain_h, gain), (wk_h, wk), (wv_h, wv),
            (val_h, wown.at[:, 0:256]), (gate_h, wown.at[:, 256:512]), (wq_h, wown.at[:, 512:768]),
            (oc_h, oown.at[:, 0:256]), (oa_h, oown.at[:, 256:512]),
            (taps_h, taps), (cbias_h, cbias), (ngain_h, ngain), (nbias_h, nbias),
        ))
    ]
    for cp in loads:
        cp.start()
    row = lax.broadcasted_iota(jnp.int32, (128, 384), 0)
    col = lax.broadcasted_iota(jnp.int32, (128, 384), 1)
    mask_s[...] = jnp.where((col >= row) & (col <= row + 2 * REACH), 0.0, -1e30).astype(F32)
    for cp in loads[2:4]:
        cp.wait()
    wg[z, x, c, :, 768:896] = jnp.concatenate([wk[...], wv[...]], axis=1)
    for cp in loads[0:2]:
        cp.wait()
    t = tok[...].astype(F32)
    inv = lax.rsqrt(jnp.mean(t * t, axis=-1, keepdims=True) + 1e-06)
    normed = (t * inv * gain[...]).astype(BF16)
    tg[y, 0] = normed[:, :1024]
    tg[y, 1] = normed[:, 1024:]
    for cp in loads[4:]:
        cp.wait()

    phase("barrier")
    pl.semaphore_wait(barrier, len(greet))
    phase("start")

    def source(r, way):
        return lax.rem(z + 16 + 4 * (r // 4) + (0, -1, 1, -2 * way)[r % 4], 16)

    def sender(j):
        return {"z": along((0, -1, 1, -2 * d)[j])}

    def wblk(r, xi):
        return wg.at[source(r, d), xi, c]

    def w_far():
        for i, e in ((1, -4), (3, 4), (2, 8)):
            send(wown, wown, out_sem.at[0], r_wz.at[4 * i], {"z": along(e)})

    def w_near(i):
        blk = wblk(4 * i, x)
        for j, e in ((1, 1), (2, -1), (3, 2 * d)):
            send(blk, blk, out_sem.at[0], r_wz.at[4 * i + j], {"z": along(e)})

    def w_arrive(r):
        dev = sender(r % 4) if r % 4 else {"z": along(4 * (r // 4))}
        got(wblk(r, x), out_sem.at[0], r_wz.at[r], dev)

    groups = ((0,), (1, 2, 3), (4, 12, 8), (5, 6, 7), (13, 14, 15), (9, 10, 11))

    def group_of(r):
        return [r in g for g in groups].index(True)

    def w_side(r):
        send(wblk(r, x), wblk(r, x), out_sem.at[1], r_wx.at[r], {"x": xr})
        send(wblk(r, x), wblk(r, x), out_sem.at[1], r_wg.at[group_of(r)], {"x": xl})

    def w_relay(r):
        got(wblk(r, xl), out_sem.at[1], r_wx.at[r], {"x": xl})
        send(wblk(r, xl), wblk(r, xl), out_sem.at[1], r_wg.at[6 + group_of(r)], {"x": xr})

    def w_pairs(*gs):
        for g in gs:
            some = wg.at[0, 0 : len(groups[g]), 0]
            got(some, out_sem.at[1], r_wg.at[g], {"x": xr})
            got(some, out_sem.at[1], r_wg.at[6 + g], {"x": xl})
            for r in groups[g]:
                both = wg.at[source(r, d), :, c]
                send(both, both, out_sem.at[2], r_wp.at[0], {"c": other})

    def oblk(i, xi):
        return og.at[source(4 * i, d), xi, c]

    def o_far():
        for i, e in ((1, -4), (3, 4), (2, 8)):
            send(oown, oown, out_sem.at[12], r_oz.at[i], {"z": along(e)})

    def o_side(i):
        if i:
            got(oblk(i, x), out_sem.at[12], r_oz.at[i], {"z": along(4 * i)})
        send(oblk(i, x), oblk(i, x), out_sem.at[3], r_ox.at[i], {"x": xr})
        send(oblk(i, x), oblk(i, x), out_sem.at[3], r_ox.at[4 + i], {"x": xl})

    def o_relay(i):
        got(oblk(i, xl), out_sem.at[3], r_ox.at[i], {"x": xl})
        send(oblk(i, xl), oblk(i, xl), out_sem.at[3], r_ox.at[8 + i], {"x": xr})

    def o_pair(r):
        four = og.at[source(r, d), :, c]
        send(four, four, out_sem.at[5], r_op.at[0], {"c": other})

    def o_near(i):
        got(oblk(i, xr), out_sem.at[3], r_ox.at[4 + i], {"x": xr})
        got(oblk(i, x2), out_sem.at[3], r_ox.at[8 + i], {"x": xl})
        four = og.at[source(4 * i, d), :, c]
        for j, e in ((1, 1), (2, -1), (3, 2 * d)):
            send(four, four, out_sem.at[4], r_on.at[i], {"z": along(e)})
        o_pair(4 * i)

    def o_last(i):
        got(og.at[0:3, :, 0], out_sem.at[4], r_on.at[i], sender(1))
        for j in (1, 2, 3):
            o_pair(4 * i + j)

    o_plan = (
        (o_far, lambda: o_side(0)),
        (lambda: o_side(1), lambda: o_side(3)),
        (lambda: o_side(2), lambda: o_near(0)),
        (lambda: o_relay(1), lambda: o_relay(3), lambda: o_relay(2)),
        (lambda: o_near(1), lambda: o_near(3)),
        (lambda: o_near(2),),
        (lambda: o_last(0),),
        (lambda: o_last(1), lambda: o_last(3)),
        (lambda: o_last(2),),
    )

    def o_step(n):
        for act in o_plan[n]:
            act()

    def w_arrivals(*rs):
        for r in rs:
            w_arrive(r)
            if r % 4 == 0:
                w_near(r // 4)
            w_side(r)

    def w_relays(*rs):
        for r in rs:
            w_relay(r)

    w_near(0)
    w_side(0)
    w_far()
    send(tg.at[y, 0], tg.at[y, 0], out_sem.at[6], r_t.at[0], {"y": yp})
    send(tg.at[y, 1], tg.at[y, 1], out_sem.at[6], r_t.at[1], {"y": ym})
    send(tg.at[y, 1], tg.at[y, 1], out_sem.at[6], r_t.at[2], {"y": yp})
    send(tg.at[y, 0], tg.at[y, 0], out_sem.at[6], r_t.at[3], {"y": ym})
    phase("arrA")
    w_arrivals(1, 2, 3)
    phase("relB")
    w_relays(0)
    phase("arrC")
    w_arrivals(4, 12)
    o_step(0)
    phase("arrE")
    w_arrivals(8)
    phase("relF")
    w_relays(1, 2, 3)
    o_relay(0)
    phase("arrH")
    w_arrivals(5, 6, 7, 13, 14, 15)
    phase("tok")
    got(tg.at[ym, 0], out_sem.at[6], r_t.at[0], {"y": ym})
    send(tg.at[ym, 0], tg.at[ym, 0], out_sem.at[6], r_t.at[4], {"y": yp})
    got(tg.at[yp, 1], out_sem.at[6], r_t.at[1], {"y": yp})
    send(tg.at[yp, 1], tg.at[yp, 1], out_sem.at[6], r_t.at[5], {"y": ym})
    phase("relI")
    w_relays(4, 12, 8)
    phase("arrK")
    w_arrivals(9, 10, 11)
    phase("o1")
    o_step(1)
    phase("pairL")
    w_pairs(0, 1)
    phase("relL")
    w_relays(5, 6, 7, 13, 14, 15)
    phase("o2")
    o_step(2)
    phase("pairM")
    w_pairs(2)
    phase("relM")
    w_relays(9, 10, 11)
    phase("pairN")
    w_pairs(3, 4)
    phase("o3")
    o_step(3)
    phase("pairO")
    w_pairs(5)
    phase("o4")
    o_step(4)
    phase("waitpair")
    got(wg.at[0:8], out_sem.at[2], r_wp.at[0], {"c": other})
    phase("waittok")
    got(tg.at[ym, 1], out_sem.at[6], r_t.at[2], {"y": ym})
    got(tg.at[yp, 0], out_sem.at[6], r_t.at[3], {"y": yp})
    got(tg.at[y2, 0], out_sem.at[6], r_t.at[4], {"y": ym})
    got(tg.at[y2, 1], out_sem.at[6], r_t.at[5], {"y": yp})
    o_left = list(range(5, len(o_plan)))

    def o_service(count=1):
        for _ in range(count):
            if o_left:
                o_step(o_left.pop(0))

    phase("proj")
    rows = 512
    ta = tg[:, 0].reshape(rows, 1024)
    tb = tg[:, 1].reshape(rows, 1024)

    def project(lo, hi):
        wa = wg[0:8, :, :, :, lo:hi].reshape(1024, hi - lo)
        wb = wg[8:16, :, :, :, lo:hi].reshape(1024, hi - lo)
        return jnp.dot(ta, wa, preferred_element_type=F32) + jnp.dot(tb, wb, preferred_element_type=F32)

    qkv = project(512, 896)
    kv_s[REACH : REACH + rows] = qkv[:, 256:].astype(BF16)
    q_s[...] = (qkv[:, :256] * 0.125).astype(BF16)
    phase("service1")
    o_service()
    phase("projglu")
    send(kv_s.at[128:256], kv_s.at[640:768], out_sem.at[11], r_h.at[2], at_sp(prv))
    send(kv_s.at[512:640], kv_s.at[0:128], out_sem.at[11], r_h.at[3], at_sp(nxt))
    glu = (project(0, 256) * jax.nn.sigmoid(project(256, 512))).astype(BF16)
    glu_s[16 : 16 + rows] = glu
    for l in range(2):
        padf[l, 16:528] = glu[:, 128 * l : 128 * l + 128].astype(F32)
    phase("service2")
    o_service()
    send(glu_s.at[16:32], glu_s.at[528:544], out_sem.at[7], r_h.at[0], at_sp(prv))
    send(glu_s.at[512:528], glu_s.at[0:16], out_sem.at[7], r_h.at[1], at_sp(nxt))

    lane64 = lax.broadcasted_iota(jnp.int32, (64, 128), 1)

    def conv_rows(i, carry):
        r0 = i * 64
        accs = []
        for l in range(2):
            lanes = slice(128 * l, 128 * l + 128)
            acc = jnp.broadcast_to(cbias[0:1, lanes], (64, 128))
            for j in range(2 * HALF + 1):
                acc = acc + padf[l, pl.ds(r0 + j + 1, 64), :] * taps[j : j + 1, lanes]
            filt[pl.ds(r0, 64), lanes] = acc
            accs.append(acc)
        s1 = jnp.sum(accs[0] + accs[1], axis=1, keepdims=True)
        s2 = jnp.sum(accs[0] * accs[0] + accs[1] * accs[1], axis=1, keepdims=True)
        stat[pl.ds(r0, 64), :] = jnp.where(lane64 == 0, s1, jnp.where(lane64 == 1, s2, 0.0))
        return carry

    phase("conv")
    lax.fori_loop(1, 7, conv_rows, 0)
    phase("service3")
    o_service()
    phase("waithalo")
    got(glu_s.at[528:544], out_sem.at[7], r_h.at[0], at_sp(nxt))
    got(glu_s.at[0:16], out_sem.at[7], r_h.at[1], at_sp(prv))
    phase("conv2")
    first = (me > 0).astype(F32)
    last = (me < 127).astype(F32)
    for l in range(2):
        lanes = slice(128 * l, 128 * l + 128)
        padf[l, 0:16] = glu_s[0:16, lanes].astype(F32) * first
        padf[l, 528:544] = glu_s[528:544, lanes].astype(F32) * last
    conv_rows(0, 0)
    conv_rows(7, 0)
    st_tx[...] = jnp.transpose(stat[...])[0:8, :]

    phase("waitkv")
    got(kv_s.at[640:768], out_sem.at[11], r_h.at[2], at_sp(nxt))
    got(kv_s.at[0:128], out_sem.at[11], r_h.at[3], at_sp(prv))
    for i, dev in enumerate((yp, ym, y2)):
        send(st_tx, st_rx.at[i], out_sem.at[8], r_st.at[0], {"y": dev})
    phase("kvprep")
    kvf = kv_s[...].astype(F32)
    turned = pltpu.roll(kvf, 64, 1)
    low = lax.broadcasted_iota(jnp.int32, (768, 128), 1) < 64
    kvw[0] = jnp.where(low, kvf, 0.0).astype(BF16)
    kvw[1] = jnp.where(low, 0.0, turned).astype(BF16)
    kvw[2] = jnp.where(low, turned, 0.0).astype(BF16)
    kvw[3] = jnp.where(low, 0.0, kvf).astype(BF16)

    phase("attend")
    low128 = lax.broadcasted_iota(jnp.int32, (128, 128), 1) < 64
    ends = lax.broadcasted_iota(jnp.int32, (1, 384), 1)

    def attend(i):
        q0 = pl.multiple_of(i * 128, 128)
        pos = me * 512 + i * 128 - REACH + ends
        edge = jnp.where((pos >= 0) & (pos < 65536), 0.0, -1e30).astype(F32)
        bias = mask_s[...] + edge
        for p in range(2):
            qp = q_s[pl.ds(q0, 128), 128 * p : 128 * p + 128]
            probs, inverse = [], []
            for b in range(2):
                h = 2 * p + b
                s = nt_dot(qp, kvw[b, pl.ds(q0, 384), :]) + bias
                top = jnp.maximum(jnp.max(s, axis=1, keepdims=True), sink[h])
                e = jnp.exp(s - top)
                total = jnp.sum(e, axis=1, keepdims=True) + jnp.exp(sink[h] - top)
                lstat[pl.ds(q0, 128), h : h + 1] = top + jnp.log(total)
                probs.append(e.astype(BF16))
                inverse.append(1.0 / total)
            o = jnp.dot(probs[0], kvw[2, pl.ds(q0, 384), :], preferred_element_type=F32)
            o = o + jnp.dot(probs[1], kvw[3, pl.ds(q0, 384), :], preferred_element_type=F32)
            o = o * jnp.where(low128, inverse[0], inverse[1])
            feat[pl.ds(q0, 128), 256 + 128 * p : 384 + 128 * p] = o.astype(BF16)

    order = (y2, yp, ym, y)
    for n in range(3):
        phase(f"attend{n}")
        attend(order[n])
        phase(f"service{n + 4}")
        o_service()
    o_service(len(o_left))
    phase("waitstat")
    got(st_rx, out_sem.at[8], r_st.at[0], {"y": ym})
    phase("norm")
    both = st_tx[...] + st_rx[0] + st_rx[1] + st_rx[2]
    stat[...] = jnp.transpose(jnp.concatenate([both, jnp.zeros((120, 512), F32)], axis=0)) * (1.0 / 1024.0)

    def norm_rows(i):
        r0 = pl.multiple_of(i * 128, 128)
        mean = stat[pl.ds(r0, 128), 0:1]
        var = stat[pl.ds(r0, 128), 1:2] - mean * mean
        v = (filt[pl.ds(r0, 128), :] - mean) * lax.rsqrt(var + 1e-05) * ngain[...] + nbias[...]
        feat[pl.ds(r0, 128), 0:256] = (v * jax.nn.sigmoid(v)).astype(BF16)

    norm_rows(y2)

    phase("waitout")
    got(og.at[0:8], out_sem.at[5], r_op.at[0], {"c": other})

    def out_half(block, half):
        f = feat[pl.ds(pl.multiple_of(block * 128, 128), 128), :]
        return nt_dot(f, og[8 * half : 8 * half + 8].reshape(1024, 512))

    phase("outmm")
    tx2[0] = out_half(y2, 0).astype(BF16)
    tx2[1] = out_half(y2, 1).astype(BF16)
    send(tx2.at[0], rx2.at[0], out_sem.at[9], r_r2.at[0], {"y": yp})
    norm_rows(yp)
    send(tx2.at[1], rx2.at[1], out_sem.at[9], r_r2.at[1], {"y": ym})
    norm_rows(ym)
    txp[0, 1] = out_half(yp, 1).astype(BF16)
    txp[1, 0] = out_half(ym, 0).astype(BF16)
    send(txp.at[0, 1], rxp.at[0, 1], out_sem.at[10], r_rp.at[1], {"y": yp})
    part[0] = out_half(yp, 0)
    send(txp.at[1, 0], rxp.at[1, 0], out_sem.at[10], r_rp.at[2], {"y": ym})
    part[1] = out_half(ym, 1)
    phase("attendown")
    attend(y)
    norm_rows(y)
    part[2] = out_half(y, 0)
    part[3] = out_half(y, 1)
    phase("wait2")
    got(rx2.at[0], out_sem.at[9], r_r2.at[0], {"y": ym})
    txp[0, 0] = (part[0] + rx2[0].astype(F32)).astype(BF16)
    got(rx2.at[1], out_sem.at[9], r_r2.at[1], {"y": yp})
    txp[1, 1] = (part[1] + rx2[1].astype(F32)).astype(BF16)
    send(txp.at[0, 0], rxp.at[0, 0], out_sem.at[10], r_rp.at[0], {"y": yp})
    send(txp.at[1, 1], rxp.at[1, 1], out_sem.at[10], r_rp.at[3], {"y": ym})
    phase("waitfin")
    log_out[...] = jnp.transpose(lstat[...])[0:4, :]
    for a, h in ((0, 1), (1, 0), (0, 0), (1, 1)):
        got(rxp.at[a, h], out_sem.at[10], r_rp.at[2 * a + h], {"y": ym if a == 0 else yp})
    phase("final")
    for h in range(2):
        total = part[2 + h] + rxp[0, h].astype(F32) + rxp[1, h].astype(F32)
        mixed[:, 1024 * h : 1024 * h + 1024] = total.astype(BF16)
    phase("drain")
    for i, ref in enumerate((
        wg.at[0:5, 0:3, 0], wg.at[0:6], wg.at[0:8], og.at[0:3, :, 0], og.at[0:6], og.at[0:8], tg.at[0:3],
        glu_s.at[0:32], st_rx, tx2, txp, kv_s.at[0:256], og.at[0:3, 0, 0],
    )):
        copy(ref, ref, out_sem.at[i], r_wp.at[0], {"c": other}).wait_send()
    phase(None)


def on_device(
    tokens, in_gain, w_conv_val, w_conv_gate, w_query, w_key, value_weight, conv_taps, conv_bias,
    norm_gain, norm_bias, head_sink_logit, w_out_conv, w_out_attn,
):
    vm = pl.BlockSpec(memory_space=pltpu.VMEM)
    dma = pltpu.SemaphoreType.DMA
    scratch = [
        pltpu.VMEM((128, 2048), BF16),
        pltpu.VMEM((1, 2048), F32),
        pltpu.VMEM((16, 64), BF16),
        pltpu.VMEM((16, 64), BF16),
        pltpu.VMEM((31, 256), F32),
        pltpu.VMEM((1, 256), F32),
        pltpu.VMEM((1, 256), F32),
        pltpu.VMEM((1, 256), F32),
        pltpu.VMEM((16, 4, 2, 16, 896), BF16),
        pltpu.VMEM((16, 4, 2, 16, 512), BF16),
        pltpu.VMEM((4, 2, 128, 1024), BF16),
        pltpu.VMEM((544, 256), BF16),
        pltpu.VMEM((512, 256), BF16),
        pltpu.VMEM((768, 128), BF16),
        pltpu.VMEM((4, 768, 128), BF16),
        pltpu.VMEM((2, 544, 128), F32),
        pltpu.VMEM((512, 256), F32),
        pltpu.VMEM((512, 128), F32),
        pltpu.VMEM((512, 128), F32),
        pltpu.VMEM((8, 512), F32),
        pltpu.VMEM((3, 8, 512), F32),
        pltpu.VMEM((512, 512), BF16),
        pltpu.VMEM((128, 384), F32),
        pltpu.VMEM((4, 128, 1024), F32),
        pltpu.VMEM((2, 128, 1024), BF16),
        pltpu.VMEM((2, 128, 1024), BF16),
        pltpu.VMEM((2, 2, 128, 1024), BF16),
        pltpu.VMEM((2, 2, 128, 1024), BF16),
        dma((13,)),
    ]
    for n in (16, 16, 12, 1, 12, 4, 4, 1, 6, 4, 1, 2, 4, 13):
        scratch += [dma((n,))]
    mixed, log_total = pl.pallas_call(
        layer,
        name="layer",
        out_shape=(
            pltpu.VMEM((128, 2048), BF16),
            pltpu.VMEM((4, 512), F32),
        ),
        in_specs=[pl.BlockSpec(memory_space=pl.ANY)] * 13 + [pl.BlockSpec(memory_space=pltpu.SMEM)],
        out_specs=(vm, vm),
        scratch_shapes=scratch,
        compiler_params=pltpu.CompilerParams(
            collective_id=0, has_side_effects=True, vmem_limit_bytes=56 * 1024 * 1024
        ),
    )(
        tokens, in_gain[None], w_conv_val, w_conv_gate, w_query, w_key, value_weight,
        w_out_conv.T, w_out_attn.T, conv_taps, conv_bias[None], norm_gain[None], norm_bias[None],
        head_sink_logit,
    )
    return mixed, log_total.T


def solution(mesh):
    finer = Mesh(mesh.devices.reshape(16, 4, 2, mesh.shape["tp"]), ("z", "x", "c", "y"))
    in_specs = (
        P(SP_TP, None), P(),
        P(SP, "y"), P(SP, "y"), P(SP, "y"), P(SP, "y"), P(SP, "y"),
        P(None, "y"), P("y"), P("y"), P("y"), P("y"),
        P("y", SP), P("y", SP),
    )
    return jax.shard_map(
        on_device, mesh=finer, in_specs=in_specs, out_specs=(P(SP_TP, None), P(SP, "y")), check_vma=False
    )
```

```python
import jax
import jax.numpy as jnp
from jax import lax
from jax.experimental import pallas as pl
from jax.experimental.pallas import tpu as pltpu
from jax.sharding import Mesh
from jax.sharding import PartitionSpec as P

MESH = pl.DeviceIdType.MESH
REACH = 128
HEADS = 4
HALF = 15
F32 = jnp.float32
BF16 = jnp.bfloat16
SP = ("z", "x", "c")
SP_TP = ("z", "x", "c", "y")


def nt_dot(a, b):
    return lax.dot_general(a, b, (((1,), (1,)), ((), ())), preferred_element_type=F32)


def layer(
    tok_h, gain_h, val_h, gate_h, wq_h, wk_h, wv_h, oc_h, oa_h, taps_h, cbias_h, ngain_h, nbias_h, sink_h,
    mixed, log_out,
    tok, gain, wk, wv, taps, cbias, ngain, nbias, sink,
    wg, og, tg, glu_s, q_s, kv_s, kvw, padf, filt, stat, lstat, st_tx, st_rx, feat, mask_s,
    part, tx2, rx2, tx4, rx4, s_in,
    r_wz, r_wx, r_wg, r_wp, r_ox, r_oz, r_on, r_op, r_t, r_h, r_st, r_r2, r_rp, out_sem,
):
    z, x, c, y = (lax.axis_index(n) for n in ("z", "x", "c", "y"))
    d = 1 - 2 * c

    def along(e):
        return lax.rem(z + 16 + e, 16)

    xr, xl = lax.rem(x + 4 + d, 4), lax.rem(x + 4 - d, 4)
    x2 = lax.rem(x + 2, 4)
    yp, ym, y2 = lax.rem(y + 1, 4), lax.rem(y + 3, 4), lax.rem(y + 2, 4)
    other = 1 - c
    me = z * 8 + x * 2 + c
    nxt, prv = lax.rem(me + 1, 128), lax.rem(me + 127, 128)

    def at_sp(s):
        return {"z": s // 8, "x": lax.rem(s // 2, 4), "c": lax.rem(s, 2)}

    def copy(src, dst, ssem, rsem, dev):
        return pltpu.make_async_remote_copy(
            src_ref=src, dst_ref=dst, send_sem=ssem, recv_sem=rsem,
            device_id=dev, device_id_type=MESH,
        )

    open_scope = []

    def phase(name):
        if open_scope:
            open_scope.pop().__exit__(None, None, None)
        if name:
            scope = jax.named_scope(name)
            scope.__enter__()
            open_scope.append(scope)

    def send(src, dst, ssem, rsem, dev):
        copy(src, dst, ssem, rsem, dev).start()

    def got(dst, ssem, rsem, dev):
        copy(dst, dst, ssem, rsem, dev).wait_recv()

    phase("greet")
    barrier = pltpu.get_barrier_semaphore()
    greet = [{"z": along(e)} for e in (1, -1, 2, -2, 4, -4)]
    greet += [{"x": xr}, {"x": xl}, {"c": other}, {"y": yp}, {"y": ym}, {"y": y2}, at_sp(nxt), at_sp(prv)]
    for dev in greet:
        pl.semaphore_signal(barrier, inc=1, device_id=dev, device_id_type=MESH)

    wown, oown = wg.at[z, x, c], og.at[z, x, c]
    loads = [
        pltpu.make_async_copy(src, dst, s_in.at[i])
        for i, (src, dst) in enumerate((
            (tok_h, tok), (gain_h, gain), (wk_h, wk), (wv_h, wv),
            (val_h, wown.at[:, 0:256]), (gate_h, wown.at[:, 256:512]), (wq_h, wown.at[:, 512:768]),
            (oc_h, oown.at[:, 0:256]), (oa_h, oown.at[:, 256:512]),
            (taps_h, taps), (cbias_h, cbias), (ngain_h, ngain), (nbias_h, nbias), (sink_h, sink),
        ))
    ]
    for cp in loads:
        cp.start()
    row = lax.broadcasted_iota(jnp.int32, (128, 384), 0)
    col = lax.broadcasted_iota(jnp.int32, (128, 384), 1)
    mask_s[...] = jnp.where((col >= row) & (col <= row + 2 * REACH), 0.0, -1e30).astype(F32)
    for cp in loads[2:4]:
        cp.wait()
    wg[z, x, c, :, 768:896] = jnp.concatenate([wk[...], wv[...]], axis=1)
    for cp in loads[0:2]:
        cp.wait()
    t = tok[...].astype(F32)
    inv = lax.rsqrt(jnp.mean(t * t, axis=-1, keepdims=True) + 1e-06)
    normed = (t * inv * gain[...]).astype(BF16)
    tg[y, 0] = normed[:, :1024]
    tg[y, 1] = normed[:, 1024:]
    for cp in loads[4:]:
        cp.wait()

    phase("barrier")
    pl.semaphore_wait(barrier, len(greet))
    phase("start")

    def source(r, way):
        return lax.rem(z + 16 + 4 * (r // 4) + (0, -1, 1, -2 * way)[r % 4], 16)

    def sender(j):
        return {"z": along((0, -1, 1, -2 * d)[j])}

    def wblk(r, xi):
        return wg.at[source(r, d), xi, c]

    def w_far():
        for i, e in ((1, -4), (3, 4)):
            send(wown, wown, out_sem.at[0], r_wz.at[4 * i], {"z": along(e)})

    def w_farther():
        blk = wg.at[along(-4 * d), x, c]
        send(blk, blk, out_sem.at[0], r_wz.at[8], {"z": along(4 * d)})

    def w_near(i):
        blk = wblk(4 * i, x)
        for j, e in ((1, 1), (2, -1), (3, 2 * d)):
            send(blk, blk, out_sem.at[0], r_wz.at[4 * i + j], {"z": along(e)})

    def w_arrive(r):
        dev = sender(r % 4) if r % 4 else {"z": along(-4 * d) if r == 8 else along(4 * (r // 4))}
        got(wblk(r, x), out_sem.at[0], r_wz.at[r], dev)

    groups = ((0,), (1, 2, 3), (4,), (12, 8), (13, 14, 15), (9, 10, 11))

    def group_of(r):
        return [r in g for g in groups].index(True)

    def w_side(r):
        send(wblk(r, x), wblk(r, x), out_sem.at[1], r_wx.at[r], {"x": xr})
        send(wblk(r, x), wblk(r, x), out_sem.at[1], r_wg.at[group_of(r)], {"x": xl})

    def w_relay(r):
        got(wblk(r, xl), out_sem.at[1], r_wx.at[r], {"x": xl})
        send(wblk(r, xl), wblk(r, xl), out_sem.at[1], r_wg.at[6 + group_of(r)], {"x": xr})

    def w_pairs(*gs):
        for g in gs:
            some = wg.at[0, 0 : len(groups[g]), 0]
            got(some, out_sem.at[1], r_wg.at[g], {"x": xr})
            got(some, out_sem.at[1], r_wg.at[6 + g], {"x": xl})
            for r in groups[g]:
                both = wg.at[source(r, d), :, c]
                send(both, both, out_sem.at[2], r_wp.at[0], {"c": other})

    def oblk(i, xi):
        return og.at[source(4 * i, d), xi, c]

    def o_far():
        for i, e in ((1, -4), (3, 4)):
            send(oown, oown, out_sem.at[12], r_oz.at[i], {"z": along(e)})

    def o_farther():
        blk = og.at[along(-4 * d), x, c]
        send(blk, blk, out_sem.at[12], r_oz.at[2], {"z": along(4 * d)})

    def o_side(i):
        if i:
            got(oblk(i, x), out_sem.at[12], r_oz.at[i], {"z": along(-4 * d) if i == 2 else along(4 * i)})
        send(oblk(i, x), oblk(i, x), out_sem.at[3], r_ox.at[i], {"x": xr})
        send(oblk(i, x), oblk(i, x), out_sem.at[3], r_ox.at[4 + i], {"x": xl})

    def o_relay(i):
        got(oblk(i, xl), out_sem.at[3], r_ox.at[i], {"x": xl})
        send(oblk(i, xl), oblk(i, xl), out_sem.at[3], r_ox.at[8 + i], {"x": xr})

    def o_pair(r):
        four = og.at[source(r, d), :, c]
        send(four, four, out_sem.at[5], r_op.at[4 if r % 4 == 3 else r // 4], {"c": other})

    def o_near(i):
        got(oblk(i, xr), out_sem.at[3], r_ox.at[4 + i], {"x": xr})
        got(oblk(i, x2), out_sem.at[3], r_ox.at[8 + i], {"x": xl})
        four = og.at[source(4 * i, d), :, c]
        for j, e in ((1, 1), (2, -1), (3, 2 * d)):
            send(four, four, out_sem.at[4], r_on.at[i], {"z": along(e)})
        o_pair(4 * i)

    def o_last(i):
        got(og.at[0:3, :, 0], out_sem.at[4], r_on.at[i], sender(1))
        for j in (1, 2, 3):
            o_pair(4 * i + j)

    o_plan = (
        (o_far, lambda: o_side(0)),
        (lambda: o_side(1), lambda: o_side(3), o_farther),
        (),
        (lambda: o_relay(1), lambda: o_relay(3)),
        (lambda: o_relay(2),),
        (lambda: o_last(0),),
        (lambda: o_near(2),),
        (lambda: o_last(1), lambda: o_last(3)),
        (lambda: o_last(2),),
    )

    def o_step(n):
        for act in o_plan[n]:
            act()

    def w_arrivals(*rs):
        for r in rs:
            w_arrive(r)
            if r == 12:
                w_farther()
            if r in (8, 12):
                w_near(r // 4)
            w_side(r)

    def w_bundle():
        four = wg.at[source(4, d), :, c]
        for j, e in ((1, 1), (2, -1), (3, 2 * d)):
            send(four, four, out_sem.at[0], r_wz.at[4 + j], {"z": along(e)})

    def w_bundles_in():
        for r in (5, 6, 7):
            four = wg.at[source(r, d), :, c]
            got(four, out_sem.at[0], r_wz.at[r], sender(r % 4))
            send(four, four, out_sem.at[2], r_wp.at[0], {"c": other})

    def w_relays(*rs):
        for r in rs:
            w_relay(r)

    w_near(0)
    w_side(0)
    w_far()
    send(tg.at[y, 0], tg.at[y, 0], out_sem.at[6], r_t.at[0], {"y": yp})
    send(tg.at[y, 1], tg.at[y, 1], out_sem.at[6], r_t.at[1], {"y": ym})
    send(tg.at[y, 1], tg.at[y, 1], out_sem.at[6], r_t.at[2], {"y": yp})
    send(tg.at[y, 0], tg.at[y, 0], out_sem.at[6], r_t.at[3], {"y": ym})
    phase("arrA")
    w_arrivals(1, 2, 3)
    phase("relB")
    w_relays(0)
    phase("arrC")
    w_arrive(4)
    w_arrivals(12)
    w_side(4)
    o_step(0)
    phase("relF")
    w_relays(1, 2, 3, 4)
    phase("arrE")
    w_arrivals(8)
    o_relay(0)
    phase("arrH")
    w_arrivals(13, 14, 15)
    phase("tok")
    got(tg.at[ym, 0], out_sem.at[6], r_t.at[0], {"y": ym})
    send(tg.at[ym, 0], tg.at[ym, 0], out_sem.at[6], r_t.at[4], {"y": yp})
    got(tg.at[yp, 1], out_sem.at[6], r_t.at[1], {"y": yp})
    send(tg.at[yp, 1], tg.at[yp, 1], out_sem.at[6], r_t.at[5], {"y": ym})
    phase("pairK")
    w_pairs(2)
    w_bundle()
    phase("o1")
    o_step(1)
    phase("relI")
    w_relays(12, 8)
    phase("arrK")
    w_arrivals(9, 10, 11)
    phase("pairL")
    w_pairs(0, 1)
    phase("relL")
    w_relays(13, 14, 15)
    phase("o2")
    o_near(0)
    phase("pairM")
    w_pairs(3)
    phase("relM")
    w_relays(9, 10, 11)
    phase("o3")
    o_step(3)
    phase("pairN")
    w_pairs(4)
    phase("bundin")
    w_bundles_in()
    phase("o3b")
    o_side(2)
    phase("pairO")
    w_pairs(5)
    phase("o4")
    o_near(1)
    o_near(3)
    phase("waitpair")
    got(wg.at[0:8], out_sem.at[2], r_wp.at[0], {"c": other})
    phase("waittok")
    got(tg.at[ym, 1], out_sem.at[6], r_t.at[2], {"y": ym})
    got(tg.at[yp, 0], out_sem.at[6], r_t.at[3], {"y": yp})
    got(tg.at[y2, 0], out_sem.at[6], r_t.at[4], {"y": ym})
    got(tg.at[y2, 1], out_sem.at[6], r_t.at[5], {"y": yp})
    o_left = list(range(4, len(o_plan)))

    def o_service(count=1):
        for _ in range(count):
            if o_left:
                o_step(o_left.pop(0))

    phase("proj")
    rows = 512
    ta = tg[:, 0].reshape(rows, 1024)
    tb = tg[:, 1].reshape(rows, 1024)

    def project(lo, hi):
        wa = wg[0:8, :, :, :, lo:hi].reshape(1024, hi - lo)
        wb = wg[8:16, :, :, :, lo:hi].reshape(1024, hi - lo)
        return jnp.dot(ta, wa, preferred_element_type=F32) + jnp.dot(tb, wb, preferred_element_type=F32)

    glu = (project(0, 256) * jax.nn.sigmoid(project(256, 512))).astype(BF16)
    glu_s[16 : 16 + rows] = glu
    for l in range(2):
        padf[l, 16:528] = glu[:, 128 * l : 128 * l + 128].astype(F32)
    send(glu_s.at[16:32], glu_s.at[528:544], out_sem.at[7], r_h.at[0], at_sp(prv))
    send(glu_s.at[512:528], glu_s.at[0:16], out_sem.at[7], r_h.at[1], at_sp(nxt))
    phase("service1")
    o_service()
    phase("projqkv")
    qkv = project(512, 896)
    kv_s[REACH : REACH + rows] = qkv[:, 256:].astype(BF16)
    q_s[...] = (qkv[:, :256] * 0.125).astype(BF16)
    send(kv_s.at[128:256], kv_s.at[640:768], out_sem.at[11], r_h.at[2], at_sp(prv))
    send(kv_s.at[512:640], kv_s.at[0:128], out_sem.at[11], r_h.at[3], at_sp(nxt))
    phase("service2")
    o_service()

    lane64 = lax.broadcasted_iota(jnp.int32, (64, 128), 1)

    def conv_rows(i, carry):
        r0 = i * 64
        accs = []
        for l in range(2):
            lanes = slice(128 * l, 128 * l + 128)
            acc = jnp.broadcast_to(cbias[0:1, lanes], (64, 128))
            for j in range(2 * HALF + 1):
                acc = acc + padf[l, pl.ds(r0 + j + 1, 64), :] * taps[j : j + 1, lanes]
            filt[pl.ds(r0, 64), lanes] = acc
            accs.append(acc)
        s1 = jnp.sum(accs[0] + accs[1], axis=1, keepdims=True)
        s2 = jnp.sum(accs[0] * accs[0] + accs[1] * accs[1], axis=1, keepdims=True)
        stat[pl.ds(r0, 64), :] = jnp.where(lane64 == 0, s1, jnp.where(lane64 == 1, s2, 0.0))
        return carry

    phase("conv")
    lax.fori_loop(1, 7, conv_rows, 0)
    phase("service3")
    o_service()
    phase("waithalo")
    got(glu_s.at[528:544], out_sem.at[7], r_h.at[0], at_sp(nxt))
    got(glu_s.at[0:16], out_sem.at[7], r_h.at[1], at_sp(prv))
    phase("conv2")
    first = (me > 0).astype(F32)
    last = (me < 127).astype(F32)
    for l in range(2):
        lanes = slice(128 * l, 128 * l + 128)
        padf[l, 0:16] = glu_s[0:16, lanes].astype(F32) * first
        padf[l, 528:544] = glu_s[528:544, lanes].astype(F32) * last
    conv_rows(0, 0)
    conv_rows(7, 0)
    st_tx[...] = jnp.transpose(stat[...])[0:8, :]

    phase("waitkv")
    got(kv_s.at[640:768], out_sem.at[11], r_h.at[2], at_sp(nxt))
    got(kv_s.at[0:128], out_sem.at[11], r_h.at[3], at_sp(prv))
    for i, dev in enumerate((yp, ym, y2)):
        send(st_tx, st_rx.at[i], out_sem.at[8], r_st.at[0], {"y": dev})
    phase("kvprep")
    kvf = kv_s[...].astype(F32)
    turned = pltpu.roll(kvf, 64, 1)
    low = lax.broadcasted_iota(jnp.int32, (768, 128), 1) < 64
    kvw[0] = jnp.where(low, kvf, 0.0).astype(BF16)
    kvw[1] = jnp.where(low, 0.0, turned).astype(BF16)
    kvw[2] = jnp.where(low, turned, 0.0).astype(BF16)
    kvw[3] = jnp.where(low, 0.0, kvf).astype(BF16)

    phase("attend")
    low128 = lax.broadcasted_iota(jnp.int32, (128, 128), 1) < 64
    ends = lax.broadcasted_iota(jnp.int32, (1, 384), 1)

    def attend(i):
        q0 = pl.multiple_of(i * 128, 128)
        pos = me * 512 + i * 128 - REACH + ends
        edge = jnp.where((pos >= 0) & (pos < 65536), 0.0, -1e30).astype(F32)
        bias = mask_s[...] + edge
        for p in range(2):
            qp = q_s[pl.ds(q0, 128), 128 * p : 128 * p + 128]
            probs, inverse = [], []
            for b in range(2):
                h = 2 * p + b
                s = nt_dot(qp, kvw[b, pl.ds(q0, 384), :]) + bias
                top = jnp.maximum(jnp.max(s, axis=1, keepdims=True), sink[h])
                e = jnp.exp(s - top)
                total = jnp.sum(e, axis=1, keepdims=True) + jnp.exp(sink[h] - top)
                lstat[pl.ds(q0, 128), h : h + 1] = top + jnp.log(total)
                probs.append(e.astype(BF16))
                inverse.append(1.0 / total)
            o = jnp.dot(probs[0], kvw[2, pl.ds(q0, 384), :], preferred_element_type=F32)
            o = o + jnp.dot(probs[1], kvw[3, pl.ds(q0, 384), :], preferred_element_type=F32)
            o = o * jnp.where(low128, inverse[0], inverse[1])
            feat[pl.ds(q0, 128), 256 + 128 * p : 384 + 128 * p] = o.astype(BF16)

    order = (y2, yp, ym, y)
    for n in range(3):
        phase(f"attend{n}")
        attend(order[n])
        if n == 1:
            phase("service4")
            o_service()
    phase("waitstat")
    got(st_rx, out_sem.at[8], r_st.at[0], {"y": ym})
    phase("norm")
    both = st_tx[...] + st_rx[0] + st_rx[1] + st_rx[2]
    stat[...] = jnp.transpose(jnp.concatenate([both, jnp.zeros((120, 512), F32)], axis=0)) * (1.0 / 1024.0)

    def norm_rows(i):
        r0 = pl.multiple_of(i * 128, 128)
        mean = stat[pl.ds(r0, 128), 0:1]
        var = stat[pl.ds(r0, 128), 1:2] - mean * mean
        v = (filt[pl.ds(r0, 128), :] - mean) * lax.rsqrt(var + 1e-05) * ngain[...] + nbias[...]
        feat[pl.ds(r0, 128), 0:256] = (v * jax.nn.sigmoid(v)).astype(BF16)

    norm_rows(y2)

    def zcol(i, j):
        return lax.rem(z + 16 + 4 * i + (0, -1, 1, 2)[j], 16)

    ups = ([(0, 0), (0, 2)], [(1, 0)], [(3, 0), (3, 2)], [(2, 0)], [(0, 3), (1, 3)])
    downs = ([(0, 1)], [(1, 1), (1, 2)], [(3, 1)], [(2, 1), (2, 2)], [(2, 3), (3, 3)])
    u_at, d_at = (0, 2, 3, 5, 6, 8), (0, 1, 3, 4, 6, 8)

    def out_group(block, n):
        f = feat[pl.ds(pl.multiple_of(block * 128, 128), 128), :]
        w = jnp.concatenate([og[zcol(i, j)].reshape(128, 512) for i, j in ups[n] + downs[n]], axis=0)
        v = nt_dot(f, w)
        cut = [v[:, 128 * k : 128 * k + 128] for k in range(len(ups[n]) + len(downs[n]))]
        return cut[: len(ups[n])], cut[len(ups[n]) :]

    def put(ref, first, blocks):
        for k, v in enumerate(blocks):
            ref[first + k] = v.astype(ref.dtype)

    def columns_here(n):
        if n < 4:
            got(og.at[0:3, :, 0], out_sem.at[5], r_op.at[(0, 1, 3, 2)[n]], {"c": other})
        else:
            got(og.at[0:2], out_sem.at[5], r_op.at[4], {"c": other})

    def send_far(n):
        us, ds = pl.ds(u_at[n], len(ups[n])), pl.ds(d_at[n], len(downs[n]))
        send(tx2.at[0, us], rx2.at[0, us], out_sem.at[9], r_r2.at[n], {"y": yp})
        send(tx2.at[1, ds], rx2.at[1, ds], out_sem.at[9], r_r2.at[5 + n], {"y": ym})

    def far_group(n):
        phase(f"waitout{n}")
        columns_here(n)
        phase(f"far{n}")
        u, dn = out_group(y2, n)
        put(tx2.at[0], u_at[n], u)
        put(tx2.at[1], d_at[n], dn)

    far_group(0)
    far_group(1)
    send_far(0)
    far_group(2)
    send_far(1)
    norm_rows(yp)
    send_far(2)
    norm_rows(ym)
    phase("service7")
    o_service(len(o_left))
    far_group(3)
    far_group(4)
    send_far(3)
    phase("near")
    for n in range(5):
        u, dn = out_group(yp, n)
        put(part.at[0], u_at[n], u)
        put(tx4.at[0, 1], d_at[n], dn)
        if n == 0:
            send_far(4)
    for n in range(5):
        u, dn = out_group(ym, n)
        put(tx4.at[1, 0], u_at[n], u)
        put(part.at[1], d_at[n], dn)
        if n == 0:
            send(tx4.at[0, 1], rx4.at[0, 1], out_sem.at[10], r_rp.at[0], {"y": yp})
    phase("attendown")
    attend(y)
    send(tx4.at[1, 0], rx4.at[1, 0], out_sem.at[10], r_rp.at[1], {"y": ym})
    norm_rows(y)
    for n in range(5):
        u, dn = out_group(y, n)
        put(part.at[2], u_at[n], u)
        put(part.at[3], d_at[n], dn)

    def send_near(n):
        us, ds = pl.ds(u_at[n], len(ups[n])), pl.ds(d_at[n], len(downs[n]))
        send(tx4.at[0, 0, us], rx4.at[0, 0, us], out_sem.at[10], r_rp.at[2], {"y": yp})
        send(tx4.at[1, 1, ds], rx4.at[1, 1, ds], out_sem.at[10], r_rp.at[3], {"y": ym})

    phase("wait2")
    for n in range(5):
        us, ds = pl.ds(u_at[n], len(ups[n])), pl.ds(d_at[n], len(downs[n]))
        got(rx2.at[0, us], out_sem.at[9], r_r2.at[n], {"y": ym})
        tx4[0, 0, us] = (part[0, us] + rx2[0, us].astype(F32)).astype(BF16)
        got(rx2.at[1, ds], out_sem.at[9], r_r2.at[5 + n], {"y": yp})
        tx4[1, 1, ds] = (part[1, ds] + rx2[1, ds].astype(F32)).astype(BF16)
        if n:
            send_near(n - 1)
    phase("waitfin")
    log_out[...] = jnp.transpose(lstat[...])[0:4, :]
    send_near(4)
    got(rx4.at[0, 1], out_sem.at[10], r_rp.at[0], {"y": ym})
    got(rx4.at[1, 0], out_sem.at[10], r_rp.at[1], {"y": yp})
    got(rx4.at[0, 0], out_sem.at[10], r_rp.at[2], {"y": ym})
    got(rx4.at[1, 1], out_sem.at[10], r_rp.at[3], {"y": yp})
    phase("final")
    for way, at, sets in ((0, u_at, ups), (1, d_at, downs)):
        for n in range(5):
            for k, (i, j) in enumerate(sets[n]):
                p = at[n] + k
                total = part[2 + way, p] + rx4[0, way, p].astype(F32) + rx4[1, way, p].astype(F32)
                mixed[:, pl.ds(pl.multiple_of(zcol(i, j) * 128, 128), 128)] = total.astype(BF16)
    phase("drain")
    for i, ref in enumerate((
        wg.at[0:3], wg.at[0:13, 0:3, 0], wg.at[0:8], og.at[0:3, :, 0], og.at[0:6], og.at[0:8], tg.at[0:3],
        glu_s.at[0:32], st_rx, tx2, tx4, kv_s.at[0:256], og.at[0:3, 0, 0],
    )):
        copy(ref, ref, out_sem.at[i], r_wp.at[0], {"c": other}).wait_send()
    phase(None)


def on_device(
    tokens, in_gain, w_conv_val, w_conv_gate, w_query, w_key, value_weight, conv_taps, conv_bias,
    norm_gain, norm_bias, head_sink_logit, w_out_conv, w_out_attn,
):
    vm = pl.BlockSpec(memory_space=pltpu.VMEM)
    dma = pltpu.SemaphoreType.DMA
    scratch = [
        pltpu.VMEM((128, 2048), BF16),
        pltpu.VMEM((1, 2048), F32),
        pltpu.VMEM((16, 64), BF16),
        pltpu.VMEM((16, 64), BF16),
        pltpu.VMEM((31, 256), F32),
        pltpu.VMEM((1, 256), F32),
        pltpu.VMEM((1, 256), F32),
        pltpu.VMEM((1, 256), F32),
        pltpu.SMEM((4,), F32),
        pltpu.VMEM((16, 4, 2, 16, 896), BF16),
        pltpu.VMEM((16, 4, 2, 16, 512), BF16),
        pltpu.VMEM((4, 2, 128, 1024), BF16),
        pltpu.VMEM((544, 256), BF16),
        pltpu.VMEM((512, 256), BF16),
        pltpu.VMEM((768, 128), BF16),
        pltpu.VMEM((4, 768, 128), BF16),
        pltpu.VMEM((2, 544, 128), F32),
        pltpu.VMEM((512, 256), F32),
        pltpu.VMEM((512, 128), F32),
        pltpu.VMEM((512, 128), F32),
        pltpu.VMEM((8, 512), F32),
        pltpu.VMEM((3, 8, 512), F32),
        pltpu.VMEM((512, 512), BF16),
        pltpu.VMEM((128, 384), F32),
        pltpu.VMEM((4, 8, 128, 128), F32),
        pltpu.VMEM((2, 8, 128, 128), BF16),
        pltpu.VMEM((2, 8, 128, 128), BF16),
        pltpu.VMEM((2, 2, 8, 128, 128), BF16),
        pltpu.VMEM((2, 2, 8, 128, 128), BF16),
        dma((14,)),
    ]
    for n in (16, 16, 12, 1, 12, 4, 4, 5, 6, 4, 1, 10, 4, 13):
        scratch += [dma((n,))]
    mixed, log_total = pl.pallas_call(
        layer,
        name="layer",
        out_shape=(
            pltpu.VMEM((128, 2048), BF16),
            pltpu.VMEM((4, 512), F32),
        ),
        in_specs=[pl.BlockSpec(memory_space=pl.ANY)] * 14,
        out_specs=(vm, vm),
        scratch_shapes=scratch,
        compiler_params=pltpu.CompilerParams(
            collective_id=0, has_side_effects=True, vmem_limit_bytes=56 * 1024 * 1024
        ),
    )(
        tokens, in_gain[None], w_conv_val, w_conv_gate, w_query, w_key, value_weight,
        w_out_conv.T, w_out_attn.T, conv_taps, conv_bias[None], norm_gain[None], norm_bias[None],
        head_sink_logit,
    )
    return mixed, log_total.T


def solution(mesh):
    finer = Mesh(mesh.devices.reshape(16, 4, 2, mesh.shape["tp"]), ("z", "x", "c", "y"))
    in_specs = (
        P(SP_TP, None), P(),
        P(SP, "y"), P(SP, "y"), P(SP, "y"), P(SP, "y"), P(SP, "y"),
        P(None, "y"), P("y"), P("y"), P("y"), P("y"),
        P("y", SP), P("y", SP),
    )
    return jax.shard_map(
        on_device, mesh=finer, in_specs=in_specs, out_specs=(P(SP_TP, None), P(SP, "y")), check_vma=False
    )
```

```python
import jax
import jax.numpy as jnp
from jax import lax
from jax.experimental import pallas as pl
from jax.experimental.pallas import tpu as pltpu
from jax.sharding import Mesh
from jax.sharding import PartitionSpec as P

MESH = pl.DeviceIdType.MESH
REACH = 128
HEADS = 4
HALF = 15
F32 = jnp.float32
BF16 = jnp.bfloat16
SP = ("z", "x", "c")
SP_TP = ("z", "x", "c", "y")


def nt_dot(a, b):
    return lax.dot_general(a, b, (((1,), (1,)), ((), ())), preferred_element_type=F32)


def layer(
    tok_h, gain_h, val_h, gate_h, wq_h, wk_h, wv_h, oc_h, oa_h, taps_h, cbias_h, ngain_h, nbias_h, sink_h,
    mixed, log_out,
    tok, gain, wk, wv, taps, cbias, ngain, nbias, sink,
    wg, og, tg, glu_s, q_s, kv_s, kvw, padf, filt, stat, lstat, st_tx, st_rx, feat, mask_s,
    part, tx2, rx2, tx4, rx4, s_in,
    r_wz, r_wx, r_wg, r_wp, r_ox, r_oz, r_on, r_op, r_t, r_h, r_st, r_r2, r_rp, out_sem,
):
    z, x, c, y = (lax.axis_index(n) for n in ("z", "x", "c", "y"))
    d = 1 - 2 * c

    def along(e):
        return lax.rem(z + 16 + e, 16)

    xr, xl = lax.rem(x + 4 + d, 4), lax.rem(x + 4 - d, 4)
    x2 = lax.rem(x + 2, 4)
    yp, ym, y2 = lax.rem(y + 1, 4), lax.rem(y + 3, 4), lax.rem(y + 2, 4)
    other = 1 - c
    me = z * 8 + x * 2 + c
    nxt, prv = lax.rem(me + 1, 128), lax.rem(me + 127, 128)

    def at_sp(s):
        return {"z": s // 8, "x": lax.rem(s // 2, 4), "c": lax.rem(s, 2)}

    def copy(src, dst, ssem, rsem, dev):
        return pltpu.make_async_remote_copy(
            src_ref=src, dst_ref=dst, send_sem=ssem, recv_sem=rsem,
            device_id=dev, device_id_type=MESH,
        )

    open_scope = []

    def phase(name):
        if open_scope:
            open_scope.pop().__exit__(None, None, None)
        if name:
            scope = jax.named_scope(name)
            scope.__enter__()
            open_scope.append(scope)

    def send(src, dst, ssem, rsem, dev):
        copy(src, dst, ssem, rsem, dev).start()

    def got(dst, ssem, rsem, dev):
        copy(dst, dst, ssem, rsem, dev).wait_recv()

    phase("greet")
    barrier = pltpu.get_barrier_semaphore()
    greet = [{"z": along(e)} for e in (1, -1, 2, -2, 4, -4)]
    greet += [{"x": xr}, {"x": xl}, {"c": other}, {"y": yp}, {"y": ym}, {"y": y2}, at_sp(nxt), at_sp(prv)]
    for dev in greet:
        pl.semaphore_signal(barrier, inc=1, device_id=dev, device_id_type=MESH)

    wown, oown = wg.at[z, x, c], og.at[z, x, c]
    loads = [
        pltpu.make_async_copy(src, dst, s_in.at[i])
        for i, (src, dst) in enumerate((
            (tok_h, tok), (gain_h, gain), (wk_h, wk), (wv_h, wv),
            (val_h, wown.at[:, 0:256]), (gate_h, wown.at[:, 256:512]), (wq_h, wown.at[:, 512:768]),
            (oc_h, oown.at[:, 0:256]), (oa_h, oown.at[:, 256:512]),
            (taps_h, taps), (cbias_h, cbias), (ngain_h, ngain), (nbias_h, nbias), (sink_h, sink),
        ))
    ]
    for cp in loads:
        cp.start()
    row = lax.broadcasted_iota(jnp.int32, (128, 384), 0)
    col = lax.broadcasted_iota(jnp.int32, (128, 384), 1)
    mask_s[...] = jnp.where((col >= row) & (col <= row + 2 * REACH), 0.0, -1e30).astype(F32)
    for cp in loads[2:4]:
        cp.wait()
    wg[z, x, c, :, 768:896] = jnp.concatenate([wk[...], wv[...]], axis=1)
    for cp in loads[0:2]:
        cp.wait()
    t = tok[...].astype(F32)
    inv = lax.rsqrt(jnp.mean(t * t, axis=-1, keepdims=True) + 1e-06)
    normed = (t * inv * gain[...]).astype(BF16)
    tg[y, 0] = normed[:, :1024]
    tg[y, 1] = normed[:, 1024:]
    for cp in loads[4:]:
        cp.wait()

    phase("barrier")
    pl.semaphore_wait(barrier, len(greet))
    phase("start")

    def source(r, way):
        return lax.rem(z + 16 + 4 * (r // 4) + (0, -1, 1, -2 * way)[r % 4], 16)

    def sender(j):
        return {"z": along((0, -1, 1, -2 * d)[j])}

    def wblk(r, xi):
        return wg.at[source(r, d), xi, c]

    def w_far():
        for i, e in ((1, -4), (3, 4)):
            send(wown, wown, out_sem.at[0], r_wz.at[4 * i], {"z": along(e)})

    def w_farther():
        blk = wg.at[along(-4 * d), x, c]
        send(blk, blk, out_sem.at[0], r_wz.at[8], {"z": along(4 * d)})

    def w_near(i):
        blk = wblk(4 * i, x)
        for j, e in ((1, 1), (2, -1), (3, 2 * d)):
            send(blk, blk, out_sem.at[0], r_wz.at[4 * i + j], {"z": along(e)})

    def w_arrive(r):
        dev = sender(r % 4) if r % 4 else {"z": along(-4 * d) if r == 8 else along(4 * (r // 4))}
        got(wblk(r, x), out_sem.at[0], r_wz.at[r], dev)

    def w_last_early():
        got(wg.at[0, 0:3, 0], out_sem.at[1], r_wg.at[5], {"x": xr})
        for r in groups[5]:
            for xi in (x, xl, xr):
                send(wblk(r, xi), wblk(r, xi), out_sem.at[2], r_wp.at[0], {"c": other})

    def w_last():
        got(wg.at[0, 0:3, 0], out_sem.at[1], r_wg.at[11], {"x": xl})
        for r in groups[5]:
            send(wblk(r, x2), wblk(r, x2), out_sem.at[2], r_wp.at[0], {"c": other})

    groups = ((0,), (1, 2, 3), (4,), (12, 8), (13, 14, 15), (9, 10, 11))

    def group_of(r):
        return [r in g for g in groups].index(True)

    def w_side(r):
        send(wblk(r, x), wblk(r, x), out_sem.at[1], r_wx.at[r], {"x": xr})
        send(wblk(r, x), wblk(r, x), out_sem.at[1], r_wg.at[group_of(r)], {"x": xl})

    def w_relay(r):
        got(wblk(r, xl), out_sem.at[1], r_wx.at[r], {"x": xl})
        send(wblk(r, xl), wblk(r, xl), out_sem.at[1], r_wg.at[6 + group_of(r)], {"x": xr})

    def w_pairs(*gs):
        for g in gs:
            some = wg.at[0, 0 : len(groups[g]), 0]
            got(some, out_sem.at[1], r_wg.at[g], {"x": xr})
            got(some, out_sem.at[1], r_wg.at[6 + g], {"x": xl})
            for r in groups[g]:
                both = wg.at[source(r, d), :, c]
                send(both, both, out_sem.at[2], r_wp.at[0], {"c": other})

    def oblk(i, xi):
        return og.at[source(4 * i, d), xi, c]

    def o_far():
        for i, e in ((1, -4), (3, 4)):
            send(oown, oown, out_sem.at[12], r_oz.at[i], {"z": along(e)})

    def o_farther():
        blk = og.at[along(-4 * d), x, c]
        send(blk, blk, out_sem.at[12], r_oz.at[2], {"z": along(4 * d)})

    def o_side(i):
        if i:
            got(oblk(i, x), out_sem.at[12], r_oz.at[i], {"z": along(-4 * d) if i == 2 else along(4 * i)})
        send(oblk(i, x), oblk(i, x), out_sem.at[3], r_ox.at[i], {"x": xr})
        send(oblk(i, x), oblk(i, x), out_sem.at[3], r_ox.at[4 + i], {"x": xl})

    def o_relay(i):
        got(oblk(i, xl), out_sem.at[3], r_ox.at[i], {"x": xl})
        send(oblk(i, xl), oblk(i, xl), out_sem.at[3], r_ox.at[8 + i], {"x": xr})

    def o_pair(r):
        four = og.at[source(r, d), :, c]
        send(four, four, out_sem.at[5], r_op.at[4 if r % 4 == 3 else r // 4], {"c": other})

    def o_near(i):
        got(oblk(i, xr), out_sem.at[3], r_ox.at[4 + i], {"x": xr})
        got(oblk(i, x2), out_sem.at[3], r_ox.at[8 + i], {"x": xl})
        four = og.at[source(4 * i, d), :, c]
        for j, e in ((1, 1), (2, -1), (3, 2 * d)):
            send(four, four, out_sem.at[4], r_on.at[i], {"z": along(e)})
        o_pair(4 * i)

    def o_last(i):
        got(og.at[0:3, :, 0], out_sem.at[4], r_on.at[i], sender(1))
        for j in (1, 2, 3):
            o_pair(4 * i + j)

    o_plan = (
        (o_far, lambda: o_side(0)),
        (lambda: o_side(1), lambda: o_side(3), o_farther),
        (),
        (lambda: o_relay(1), lambda: o_relay(3)),
        (lambda: o_relay(2),),
        (lambda: o_last(0),),
        (lambda: o_near(2),),
        (lambda: o_last(1), lambda: o_last(3)),
        (lambda: o_last(2),),
    )

    def o_step(n):
        for act in o_plan[n]:
            act()

    def w_arrivals(*rs):
        for r in rs:
            w_arrive(r)
            if r == 12:
                w_farther()
            if r in (8, 12):
                w_near(r // 4)
            w_side(r)

    def w_bundle():
        four = wg.at[source(4, d), :, c]
        for j, e in ((1, 1), (2, -1), (3, 2 * d)):
            send(four, four, out_sem.at[0], r_wz.at[4 + j], {"z": along(e)})

    def w_bundles_in():
        for r in (5, 6, 7):
            four = wg.at[source(r, d), :, c]
            got(four, out_sem.at[0], r_wz.at[r], sender(r % 4))
            send(four, four, out_sem.at[2], r_wp.at[0], {"c": other})

    def w_relays(*rs):
        for r in rs:
            w_relay(r)

    w_near(0)
    w_side(0)
    w_far()
    send(tg.at[y, 0], tg.at[y, 0], out_sem.at[6], r_t.at[0], {"y": yp})
    send(tg.at[y, 1], tg.at[y, 1], out_sem.at[6], r_t.at[1], {"y": ym})
    send(tg.at[y, 1], tg.at[y, 1], out_sem.at[6], r_t.at[2], {"y": yp})
    send(tg.at[y, 0], tg.at[y, 0], out_sem.at[6], r_t.at[3], {"y": ym})
    phase("arrA")
    w_arrivals(1, 2, 3)
    phase("relB")
    w_relays(0)
    phase("arrC")
    w_arrive(4)
    w_arrivals(12)
    w_side(4)
    o_step(0)
    phase("relF")
    w_relays(1, 2, 3, 4)
    phase("arrE")
    w_arrivals(8)
    o_relay(0)
    phase("arrH")
    w_arrivals(13, 14, 15)
    phase("tok")
    got(tg.at[ym, 0], out_sem.at[6], r_t.at[0], {"y": ym})
    send(tg.at[ym, 0], tg.at[ym, 0], out_sem.at[6], r_t.at[4], {"y": yp})
    got(tg.at[yp, 1], out_sem.at[6], r_t.at[1], {"y": yp})
    send(tg.at[yp, 1], tg.at[yp, 1], out_sem.at[6], r_t.at[5], {"y": ym})
    phase("pairK")
    w_pairs(2)
    w_bundle()
    phase("o1")
    o_step(1)
    phase("relI")
    w_relays(12, 8)
    phase("arrK")
    w_arrivals(9, 10, 11)
    phase("pairL")
    w_pairs(0, 1)
    phase("relL")
    w_relays(13, 14, 15)
    phase("o2")
    o_near(0)
    phase("pairM")
    w_pairs(3)
    phase("relM")
    w_relays(9, 10, 11)
    phase("o3")
    o_step(3)
    phase("pairN")
    w_pairs(4)
    phase("bundin")
    w_bundles_in()
    phase("pairO")
    w_last_early()
    phase("o3b")
    o_side(2)
    phase("pairP")
    w_last()
    phase("o4")
    o_near(1)
    o_near(3)
    phase("waitpair")
    got(wg.at[0:8], out_sem.at[2], r_wp.at[0], {"c": other})
    phase("waittok")
    got(tg.at[ym, 1], out_sem.at[6], r_t.at[2], {"y": ym})
    got(tg.at[yp, 0], out_sem.at[6], r_t.at[3], {"y": yp})
    got(tg.at[y2, 0], out_sem.at[6], r_t.at[4], {"y": ym})
    got(tg.at[y2, 1], out_sem.at[6], r_t.at[5], {"y": yp})
    o_left = list(range(4, len(o_plan)))

    def o_service(count=1):
        for _ in range(count):
            if o_left:
                o_step(o_left.pop(0))

    phase("proj")
    rows = 512
    ta = tg[:, 0].reshape(rows, 1024)
    tb = tg[:, 1].reshape(rows, 1024)

    def project(lo, hi):
        wa = wg[0:8, :, :, :, lo:hi].reshape(1024, hi - lo)
        wb = wg[8:16, :, :, :, lo:hi].reshape(1024, hi - lo)
        return jnp.dot(ta, wa, preferred_element_type=F32) + jnp.dot(tb, wb, preferred_element_type=F32)

    glu = (project(0, 256) * jax.nn.sigmoid(project(256, 512))).astype(BF16)
    glu_s[16 : 16 + rows] = glu
    for l in range(2):
        padf[l, 16:528] = glu[:, 128 * l : 128 * l + 128].astype(F32)
    send(glu_s.at[16:32], glu_s.at[528:544], out_sem.at[7], r_h.at[0], at_sp(prv))
    send(glu_s.at[512:528], glu_s.at[0:16], out_sem.at[7], r_h.at[1], at_sp(nxt))
    phase("service1")
    o_service()
    phase("projqkv")
    qkv = project(512, 896)
    kv_s[REACH : REACH + rows] = qkv[:, 256:].astype(BF16)
    q_s[...] = (qkv[:, :256] * 0.125).astype(BF16)
    send(kv_s.at[128:256], kv_s.at[640:768], out_sem.at[11], r_h.at[2], at_sp(prv))
    send(kv_s.at[512:640], kv_s.at[0:128], out_sem.at[11], r_h.at[3], at_sp(nxt))
    phase("service2")
    o_service()

    lane64 = lax.broadcasted_iota(jnp.int32, (64, 128), 1)

    def conv_rows(i, carry):
        r0 = i * 64
        accs = []
        for l in range(2):
            lanes = slice(128 * l, 128 * l + 128)
            acc = jnp.broadcast_to(cbias[0:1, lanes], (64, 128))
            for j in range(2 * HALF + 1):
                acc = acc + padf[l, pl.ds(r0 + j + 1, 64), :] * taps[j : j + 1, lanes]
            filt[pl.ds(r0, 64), lanes] = acc
            accs.append(acc)
        s1 = jnp.sum(accs[0] + accs[1], axis=1, keepdims=True)
        s2 = jnp.sum(accs[0] * accs[0] + accs[1] * accs[1], axis=1, keepdims=True)
        stat[pl.ds(r0, 64), :] = jnp.where(lane64 == 0, s1, jnp.where(lane64 == 1, s2, 0.0))
        return carry

    phase("conv")
    lax.fori_loop(1, 7, conv_rows, 0)
    phase("service3")
    o_service()
    phase("waithalo")
    got(glu_s.at[528:544], out_sem.at[7], r_h.at[0], at_sp(nxt))
    got(glu_s.at[0:16], out_sem.at[7], r_h.at[1], at_sp(prv))
    phase("conv2")
    first = (me > 0).astype(F32)
    last = (me < 127).astype(F32)
    for l in range(2):
        lanes = slice(128 * l, 128 * l + 128)
        padf[l, 0:16] = glu_s[0:16, lanes].astype(F32) * first
        padf[l, 528:544] = glu_s[528:544, lanes].astype(F32) * last
    conv_rows(0, 0)
    conv_rows(7, 0)
    st_tx[...] = jnp.transpose(stat[...])[0:8, :]

    phase("kvprep")
    low = lax.broadcasted_iota(jnp.int32, (512, 128), 1) < 64

    def widen(r0, n):
        kvf = kv_s[r0 : r0 + n].astype(F32)
        turned = pltpu.roll(kvf, 64, 1)
        lo = low[:n]
        kvw[0, r0 : r0 + n] = jnp.where(lo, kvf, 0.0).astype(BF16)
        kvw[1, r0 : r0 + n] = jnp.where(lo, 0.0, turned).astype(BF16)
        kvw[2, r0 : r0 + n] = jnp.where(lo, turned, 0.0).astype(BF16)
        kvw[3, r0 : r0 + n] = jnp.where(lo, 0.0, kvf).astype(BF16)

    widen(128, 512)
    for i, dev in enumerate((yp, ym, y2)):
        send(st_tx, st_rx.at[i], out_sem.at[8], r_st.at[0], {"y": dev})
    phase("waitkv")
    got(kv_s.at[640:768], out_sem.at[11], r_h.at[2], at_sp(nxt))
    got(kv_s.at[0:128], out_sem.at[11], r_h.at[3], at_sp(prv))
    phase("kvprep2")
    widen(0, 128)
    widen(640, 128)

    low128 = lax.broadcasted_iota(jnp.int32, (128, 128), 1) < 64
    ends = lax.broadcasted_iota(jnp.int32, (1, 384), 1)

    def attend(i):
        q0 = pl.multiple_of(i * 128, 128)
        pos = me * 512 + i * 128 - REACH + ends
        edge = jnp.where((pos >= 0) & (pos < 65536), 0.0, -1e30).astype(F32)
        bias = mask_s[...] + edge
        for p in range(2):
            qp = q_s[pl.ds(q0, 128), 128 * p : 128 * p + 128]
            probs, inverse = [], []
            for b in range(2):
                h = 2 * p + b
                s = nt_dot(qp, kvw[b, pl.ds(q0, 384), :]) + bias
                top = jnp.maximum(jnp.max(s, axis=1, keepdims=True), sink[h])
                e = jnp.exp(s - top)
                total = jnp.sum(e, axis=1, keepdims=True) + jnp.exp(sink[h] - top)
                lstat[pl.ds(q0, 128), h : h + 1] = top + jnp.log(total)
                probs.append(e.astype(BF16))
                inverse.append(1.0 / total)
            o = jnp.dot(probs[0], kvw[2, pl.ds(q0, 384), :], preferred_element_type=F32)
            o = o + jnp.dot(probs[1], kvw[3, pl.ds(q0, 384), :], preferred_element_type=F32)
            o = o * jnp.where(low128, inverse[0], inverse[1])
            feat[pl.ds(q0, 128), 256 + 128 * p : 384 + 128 * p] = o.astype(BF16)

    order = (y2, yp, ym, y)
    for n in range(3):
        phase(f"attend{n}")
        attend(order[n])
        if n == 1:
            phase("service4")
            o_service()
    phase("waitstat")
    got(st_rx, out_sem.at[8], r_st.at[0], {"y": ym})
    phase("norm")
    both = st_tx[...] + st_rx[0] + st_rx[1] + st_rx[2]
    stat[...] = jnp.transpose(jnp.concatenate([both, jnp.zeros((120, 512), F32)], axis=0)) * (1.0 / 1024.0)

    def norm_rows(i):
        r0 = pl.multiple_of(i * 128, 128)
        mean = stat[pl.ds(r0, 128), 0:1]
        var = stat[pl.ds(r0, 128), 1:2] - mean * mean
        v = (filt[pl.ds(r0, 128), :] - mean) * lax.rsqrt(var + 1e-05) * ngain[...] + nbias[...]
        feat[pl.ds(r0, 128), 0:256] = (v * jax.nn.sigmoid(v)).astype(BF16)

    norm_rows(y2)

    def zcol(i, j):
        return lax.rem(z + 16 + 4 * i + (0, -1, 1, 2)[j], 16)

    ups = ([(0, 0), (0, 2)], [(1, 0)], [(3, 0), (3, 2)], [(2, 0)], [(0, 3), (1, 3)])
    downs = ([(0, 1)], [(1, 1), (1, 2)], [(3, 1)], [(2, 1), (2, 2)], [(2, 3), (3, 3)])
    u_at, d_at = (0, 2, 3, 5, 6, 8), (0, 1, 3, 4, 6, 8)

    def out_group(block, n):
        f = feat[pl.ds(pl.multiple_of(block * 128, 128), 128), :]
        w = jnp.concatenate([og[zcol(i, j)].reshape(128, 512) for i, j in ups[n] + downs[n]], axis=0)
        v = nt_dot(f, w)
        cut = [v[:, 128 * k : 128 * k + 128] for k in range(len(ups[n]) + len(downs[n]))]
        return cut[: len(ups[n])], cut[len(ups[n]) :]

    def put(ref, first, blocks):
        for k, v in enumerate(blocks):
            ref[first + k] = v.astype(ref.dtype)

    def columns_here(n):
        if n < 4:
            got(og.at[0:3, :, 0], out_sem.at[5], r_op.at[(0, 1, 3, 2)[n]], {"c": other})
        else:
            got(og.at[0:2], out_sem.at[5], r_op.at[4], {"c": other})

    def send_far(n):
        us, ds = pl.ds(u_at[n], len(ups[n])), pl.ds(d_at[n], len(downs[n]))
        send(tx2.at[0, us], rx2.at[0, us], out_sem.at[9], r_r2.at[n], {"y": yp})
        send(tx2.at[1, ds], rx2.at[1, ds], out_sem.at[9], r_r2.at[5 + n], {"y": ym})

    def far_group(n):
        phase(f"waitout{n}")
        columns_here(n)
        phase(f"far{n}")
        u, dn = out_group(y2, n)
        put(tx2.at[0], u_at[n], u)
        put(tx2.at[1], d_at[n], dn)

    far_group(0)
    far_group(1)
    send_far(0)
    far_group(2)
    send_far(1)
    norm_rows(yp)
    send_far(2)
    norm_rows(ym)
    phase("service7")
    o_service(len(o_left))
    far_group(3)
    far_group(4)
    send_far(3)
    phase("near")
    for n in range(5):
        u, dn = out_group(yp, n)
        put(part.at[0], u_at[n], u)
        put(tx4.at[0, 1], d_at[n], dn)
        if n == 0:
            send_far(4)
    for n in range(5):
        u, dn = out_group(ym, n)
        put(tx4.at[1, 0], u_at[n], u)
        put(part.at[1], d_at[n], dn)
        if n == 0:
            send(tx4.at[0, 1], rx4.at[0, 1], out_sem.at[10], r_rp.at[0], {"y": yp})
    phase("attendown")
    attend(y)
    send(tx4.at[1, 0], rx4.at[1, 0], out_sem.at[10], r_rp.at[1], {"y": ym})
    norm_rows(y)
    for n in range(5):
        u, dn = out_group(y, n)
        put(part.at[2], u_at[n], u)
        put(part.at[3], d_at[n], dn)

    def send_near(n):
        us, ds = pl.ds(u_at[n], len(ups[n])), pl.ds(d_at[n], len(downs[n]))
        send(tx4.at[0, 0, us], rx4.at[0, 0, us], out_sem.at[10], r_rp.at[2], {"y": yp})
        send(tx4.at[1, 1, ds], rx4.at[1, 1, ds], out_sem.at[10], r_rp.at[3], {"y": ym})

    phase("wait2")
    for n in range(5):
        us, ds = pl.ds(u_at[n], len(ups[n])), pl.ds(d_at[n], len(downs[n]))
        got(rx2.at[0, us], out_sem.at[9], r_r2.at[n], {"y": ym})
        tx4[0, 0, us] = (part[0, us] + rx2[0, us].astype(F32)).astype(BF16)
        got(rx2.at[1, ds], out_sem.at[9], r_r2.at[5 + n], {"y": yp})
        tx4[1, 1, ds] = (part[1, ds] + rx2[1, ds].astype(F32)).astype(BF16)
        if n:
            send_near(n - 1)
    phase("waitfin")
    log_out[...] = jnp.transpose(lstat[...])[0:4, :]
    send_near(4)
    got(rx4.at[0, 1], out_sem.at[10], r_rp.at[0], {"y": ym})
    got(rx4.at[1, 0], out_sem.at[10], r_rp.at[1], {"y": yp})
    got(rx4.at[0, 0], out_sem.at[10], r_rp.at[2], {"y": ym})
    got(rx4.at[1, 1], out_sem.at[10], r_rp.at[3], {"y": yp})
    phase("final")
    for way, at, sets in ((0, u_at, ups), (1, d_at, downs)):
        for n in range(5):
            for k, (i, j) in enumerate(sets[n]):
                p = at[n] + k
                total = part[2 + way, p] + rx4[0, way, p].astype(F32) + rx4[1, way, p].astype(F32)
                mixed[:, pl.ds(pl.multiple_of(zcol(i, j) * 128, 128), 128)] = total.astype(BF16)
    phase("drain")
    for i, ref in enumerate((
        wg.at[0:3], wg.at[0:13, 0:3, 0], wg.at[0:8], og.at[0:3, :, 0], og.at[0:6], og.at[0:8], tg.at[0:3],
        glu_s.at[0:32], st_rx, tx2, tx4, kv_s.at[0:256], og.at[0:3, 0, 0],
    )):
        copy(ref, ref, out_sem.at[i], r_wp.at[0], {"c": other}).wait_send()
    phase(None)


def on_device(
    tokens, in_gain, w_conv_val, w_conv_gate, w_query, w_key, value_weight, conv_taps, conv_bias,
    norm_gain, norm_bias, head_sink_logit, w_out_conv, w_out_attn,
):
    vm = pl.BlockSpec(memory_space=pltpu.VMEM)
    dma = pltpu.SemaphoreType.DMA
    scratch = [
        pltpu.VMEM((128, 2048), BF16),
        pltpu.VMEM((1, 2048), F32),
        pltpu.VMEM((16, 64), BF16),
        pltpu.VMEM((16, 64), BF16),
        pltpu.VMEM((31, 256), F32),
        pltpu.VMEM((1, 256), F32),
        pltpu.VMEM((1, 256), F32),
        pltpu.VMEM((1, 256), F32),
        pltpu.SMEM((4,), F32),
        pltpu.VMEM((16, 4, 2, 16, 896), BF16),
        pltpu.VMEM((16, 4, 2, 16, 512), BF16),
        pltpu.VMEM((4, 2, 128, 1024), BF16),
        pltpu.VMEM((544, 256), BF16),
        pltpu.VMEM((512, 256), BF16),
        pltpu.VMEM((768, 128), BF16),
        pltpu.VMEM((4, 768, 128), BF16),
        pltpu.VMEM((2, 544, 128), F32),
        pltpu.VMEM((512, 256), F32),
        pltpu.VMEM((512, 128), F32),
        pltpu.VMEM((512, 128), F32),
        pltpu.VMEM((8, 512), F32),
        pltpu.VMEM((3, 8, 512), F32),
        pltpu.VMEM((512, 512), BF16),
        pltpu.VMEM((128, 384), F32),
        pltpu.VMEM((4, 8, 128, 128), F32),
        pltpu.VMEM((2, 8, 128, 128), BF16),
        pltpu.VMEM((2, 8, 128, 128), BF16),
        pltpu.VMEM((2, 2, 8, 128, 128), BF16),
        pltpu.VMEM((2, 2, 8, 128, 128), BF16),
        dma((14,)),
    ]
    for n in (16, 16, 12, 1, 12, 4, 4, 5, 6, 4, 1, 10, 4, 13):
        scratch += [dma((n,))]
    mixed, log_total = pl.pallas_call(
        layer,
        name="layer",
        out_shape=(
            pltpu.VMEM((128, 2048), BF16),
            pltpu.VMEM((4, 512), F32),
        ),
        in_specs=[pl.BlockSpec(memory_space=pl.ANY)] * 14,
        out_specs=(vm, vm),
        scratch_shapes=scratch,
        compiler_params=pltpu.CompilerParams(
            collective_id=0, has_side_effects=True, vmem_limit_bytes=56 * 1024 * 1024
        ),
    )(
        tokens, in_gain[None], w_conv_val, w_conv_gate, w_query, w_key, value_weight,
        w_out_conv.T, w_out_attn.T, conv_taps, conv_bias[None], norm_gain[None], norm_bias[None],
        head_sink_logit,
    )
    return mixed, log_total.T


def solution(mesh):
    finer = Mesh(mesh.devices.reshape(16, 4, 2, mesh.shape["tp"]), ("z", "x", "c", "y"))
    in_specs = (
        P(SP_TP, None), P(),
        P(SP, "y"), P(SP, "y"), P(SP, "y"), P(SP, "y"), P(SP, "y"),
        P(None, "y"), P("y"), P("y"), P("y"), P("y"),
        P("y", SP), P("y", SP),
    )
    return jax.shard_map(
        on_device, mesh=finer, in_specs=in_specs, out_specs=(P(SP_TP, None), P(SP, "y")), check_vma=False
    )
```

```python
import jax
import jax.numpy as jnp
from jax import lax
from jax.experimental import pallas as pl
from jax.experimental.pallas import tpu as pltpu
from jax.sharding import Mesh
from jax.sharding import PartitionSpec as P

MESH = pl.DeviceIdType.MESH
REACH = 128
HEADS = 4
HALF = 15
F32 = jnp.float32
BF16 = jnp.bfloat16
SP = ("z", "x", "c")
SP_TP = ("z", "x", "c", "y")


def nt_dot(a, b):
    return lax.dot_general(a, b, (((1,), (1,)), ((), ())), preferred_element_type=F32)


def layer(
    tok_h, gain_h, val_h, gate_h, wq_h, wk_h, wv_h, oc_h, oa_h, taps_h, cbias_h, ngain_h, nbias_h, sink_h,
    mixed, log_out,
    tok, gain, wk, wv, taps, cbias, ngain, nbias, sink,
    wg, og, tg, glu_s, q_s, kv_s, kvw, padf, filt, stat, lstat, st_tx, st_rx, feat, mask_s,
    part, tx2, rx2, tx4, rx4, s_in,
    r_wz, r_wx, r_wg, r_wp, r_ox, r_oz, r_on, r_op, r_t, r_h, r_st, r_r2, r_rp, out_sem,
):
    z, x, c, y = (lax.axis_index(n) for n in ("z", "x", "c", "y"))
    d = 1 - 2 * c

    def along(e):
        return lax.rem(z + 16 + e, 16)

    xr, xl = lax.rem(x + 4 + d, 4), lax.rem(x + 4 - d, 4)
    x2 = lax.rem(x + 2, 4)
    yp, ym, y2 = lax.rem(y + 1, 4), lax.rem(y + 3, 4), lax.rem(y + 2, 4)
    other = 1 - c
    me = z * 8 + x * 2 + c
    nxt, prv = lax.rem(me + 1, 128), lax.rem(me + 127, 128)

    def at_sp(s):
        return {"z": s // 8, "x": lax.rem(s // 2, 4), "c": lax.rem(s, 2)}

    def copy(src, dst, ssem, rsem, dev):
        return pltpu.make_async_remote_copy(
            src_ref=src, dst_ref=dst, send_sem=ssem, recv_sem=rsem,
            device_id=dev, device_id_type=MESH,
        )

    open_scope = []

    def phase(name):
        if open_scope:
            open_scope.pop().__exit__(None, None, None)
        if name:
            scope = jax.named_scope(name)
            scope.__enter__()
            open_scope.append(scope)

    def send(src, dst, ssem, rsem, dev):
        copy(src, dst, ssem, rsem, dev).start()

    def got(dst, ssem, rsem, dev):
        copy(dst, dst, ssem, rsem, dev).wait_recv()

    phase("greet")
    barrier = pltpu.get_barrier_semaphore()
    greet = [{"z": along(e)} for e in (1, -1, 2, -2, 4, -4)]
    greet += [{"x": xr}, {"x": xl}, {"c": other}, {"y": yp}, {"y": ym}, {"y": y2}, at_sp(nxt), at_sp(prv)]
    for dev in greet:
        pl.semaphore_signal(barrier, inc=1, device_id=dev, device_id_type=MESH)

    wown, oown = wg.at[z, x, c], og.at[z, x, c]
    loads = [
        pltpu.make_async_copy(src, dst, s_in.at[i])
        for i, (src, dst) in enumerate((
            (tok_h, tok), (gain_h, gain), (wk_h, wk), (wv_h, wv),
            (val_h, wown.at[:, 0:256]), (gate_h, wown.at[:, 256:512]), (wq_h, wown.at[:, 512:768]),
            (oc_h, oown.at[:, 0:256]), (oa_h, oown.at[:, 256:512]),
            (taps_h, taps), (cbias_h, cbias), (ngain_h, ngain), (nbias_h, nbias), (sink_h, sink),
        ))
    ]
    for cp in loads:
        cp.start()
    row = lax.broadcasted_iota(jnp.int32, (128, 384), 0)
    col = lax.broadcasted_iota(jnp.int32, (128, 384), 1)
    mask_s[...] = jnp.where((col >= row) & (col <= row + 2 * REACH), 0.0, -1e30).astype(F32)
    for cp in loads[2:4]:
        cp.wait()
    wg[z, x, c, :, 768:896] = jnp.concatenate([wk[...], wv[...]], axis=1)
    for cp in loads[0:2]:
        cp.wait()
    t = tok[...].astype(F32)
    inv = lax.rsqrt(jnp.mean(t * t, axis=-1, keepdims=True) + 1e-06)
    normed = (t * inv * gain[...]).astype(BF16)
    tg[y, 0] = normed[:, :1024]
    tg[y, 1] = normed[:, 1024:]
    for cp in loads[4:]:
        cp.wait()

    phase("barrier")
    pl.semaphore_wait(barrier, len(greet))
    phase("start")

    def source(r, way):
        return lax.rem(z + 16 + 4 * (r // 4) + (0, -1, 1, -2 * way)[r % 4], 16)

    def sender(j):
        return {"z": along((0, -1, 1, -2 * d)[j])}

    def wblk(r, xi):
        return wg.at[source(r, d), xi, c]

    def w_far():
        for i, e in ((1, -4), (3, 4)):
            send(wown, wown, out_sem.at[0], r_wz.at[4 * i], {"z": along(e)})

    def w_farther():
        blk = wg.at[along(-4 * d), x, c]
        send(blk, blk, out_sem.at[0], r_wz.at[8], {"z": along(4 * d)})

    def w_near(i):
        blk = wblk(4 * i, x)
        for j, e in ((1, 1), (2, -1), (3, 2 * d)):
            send(blk, blk, out_sem.at[0], r_wz.at[4 * i + j], {"z": along(e)})

    def w_arrive(r):
        dev = sender(r % 4) if r % 4 else {"z": along(-4 * d) if r == 8 else along(4 * (r // 4))}
        got(wblk(r, x), out_sem.at[0], r_wz.at[r], dev)

    def w_last_early():
        got(wg.at[0, 0:3, 0], out_sem.at[1], r_wg.at[5], {"x": xr})
        for r in groups[5]:
            for xi in (x, xl, xr):
                send(wblk(r, xi), wblk(r, xi), out_sem.at[2], r_wp.at[0], {"c": other})

    def w_last():
        got(wg.at[0, 0:3, 0], out_sem.at[1], r_wg.at[11], {"x": xl})
        for r in groups[5]:
            send(wblk(r, x2), wblk(r, x2), out_sem.at[2], r_wp.at[0], {"c": other})

    groups = ((0,), (1, 2, 3), (4,), (12, 8), (13, 14, 15), (9, 10, 11))

    def group_of(r):
        return [r in g for g in groups].index(True)

    def w_side(r):
        send(wblk(r, x), wblk(r, x), out_sem.at[1], r_wx.at[r], {"x": xr})
        send(wblk(r, x), wblk(r, x), out_sem.at[1], r_wg.at[group_of(r)], {"x": xl})

    def w_relay(r):
        got(wblk(r, xl), out_sem.at[1], r_wx.at[r], {"x": xl})
        send(wblk(r, xl), wblk(r, xl), out_sem.at[1], r_wg.at[6 + group_of(r)], {"x": xr})

    def w_pairs(*gs):
        for g in gs:
            some = wg.at[0, 0 : len(groups[g]), 0]
            got(some, out_sem.at[1], r_wg.at[g], {"x": xr})
            got(some, out_sem.at[1], r_wg.at[6 + g], {"x": xl})
            for r in groups[g]:
                both = wg.at[source(r, d), :, c]
                send(both, both, out_sem.at[2], r_wp.at[0], {"c": other})

    def oblk(i, xi):
        return og.at[source(4 * i, d), xi, c]

    def o_far():
        for i, e in ((1, -4), (3, 4)):
            send(oown, oown, out_sem.at[12], r_oz.at[i], {"z": along(e)})

    def o_farther():
        blk = og.at[along(-4 * d), x, c]
        send(blk, blk, out_sem.at[12], r_oz.at[2], {"z": along(4 * d)})

    def o_side(i):
        if i:
            got(oblk(i, x), out_sem.at[12], r_oz.at[i], {"z": along(-4 * d) if i == 2 else along(4 * i)})
        send(oblk(i, x), oblk(i, x), out_sem.at[3], r_ox.at[i], {"x": xr})
        send(oblk(i, x), oblk(i, x), out_sem.at[3], r_ox.at[4 + i], {"x": xl})

    def o_relay(i):
        got(oblk(i, xl), out_sem.at[3], r_ox.at[i], {"x": xl})
        send(oblk(i, xl), oblk(i, xl), out_sem.at[3], r_ox.at[8 + i], {"x": xr})

    def o_pair(r):
        four = og.at[source(r, d), :, c]
        send(four, four, out_sem.at[5], r_op.at[4 if r % 4 == 3 else r // 4], {"c": other})

    def o_near(i):
        got(oblk(i, xr), out_sem.at[3], r_ox.at[4 + i], {"x": xr})
        got(oblk(i, x2), out_sem.at[3], r_ox.at[8 + i], {"x": xl})
        four = og.at[source(4 * i, d), :, c]
        for j, e in ((1, 1), (2, -1), (3, 2 * d)):
            send(four, four, out_sem.at[4], r_on.at[i], {"z": along(e)})
        o_pair(4 * i)

    def o_last(i):
        got(og.at[0:3, :, 0], out_sem.at[4], r_on.at[i], sender(1))
        for j in (1, 2, 3):
            o_pair(4 * i + j)

    o_plan = (
        (o_far, lambda: o_side(0)),
        (lambda: o_side(1), lambda: o_side(3), o_farther),
        (),
        (lambda: o_relay(1), lambda: o_relay(3)),
        (lambda: o_relay(2),),
        (lambda: o_last(0),),
        (lambda: o_near(2),),
        (lambda: o_last(1), lambda: o_last(3)),
        (lambda: o_last(2),),
    )

    def o_step(n):
        for act in o_plan[n]:
            act()

    def w_arrivals(*rs):
        for r in rs:
            w_arrive(r)
            if r == 12:
                w_farther()
            if r in (8, 12):
                w_near(r // 4)
            w_side(r)

    def w_bundle():
        four = wg.at[source(4, d), :, c]
        for j, e in ((1, 1), (2, -1), (3, 2 * d)):
            send(four, four, out_sem.at[0], r_wz.at[4 + j], {"z": along(e)})

    def w_bundles_in():
        for r in (5, 6, 7):
            four = wg.at[source(r, d), :, c]
            got(four, out_sem.at[0], r_wz.at[r], sender(r % 4))
            send(four, four, out_sem.at[2], r_wp.at[0], {"c": other})

    def w_relays(*rs):
        for r in rs:
            w_relay(r)

    w_near(0)
    w_side(0)
    w_far()
    send(tg.at[y, 0], tg.at[y, 0], out_sem.at[6], r_t.at[0], {"y": yp})
    send(tg.at[y, 1], tg.at[y, 1], out_sem.at[6], r_t.at[1], {"y": ym})
    send(tg.at[y, 1], tg.at[y, 1], out_sem.at[6], r_t.at[2], {"y": yp})
    send(tg.at[y, 0], tg.at[y, 0], out_sem.at[6], r_t.at[3], {"y": ym})
    phase("arrA")
    w_arrivals(1, 2, 3)
    phase("relB")
    w_relays(0)
    phase("arrC")
    w_arrive(4)
    w_arrivals(12)
    w_side(4)
    o_step(0)
    phase("relF")
    w_relays(1, 2, 3, 4)
    phase("arrE")
    w_arrivals(8)
    o_relay(0)
    phase("arrH")
    w_arrivals(13, 14, 15)
    phase("tok")
    got(tg.at[ym, 0], out_sem.at[6], r_t.at[0], {"y": ym})
    send(tg.at[ym, 0], tg.at[ym, 0], out_sem.at[6], r_t.at[4], {"y": yp})
    got(tg.at[yp, 1], out_sem.at[6], r_t.at[1], {"y": yp})
    send(tg.at[yp, 1], tg.at[yp, 1], out_sem.at[6], r_t.at[5], {"y": ym})
    phase("pairK")
    w_pairs(2)
    w_bundle()
    phase("o1")
    o_step(1)
    phase("relI")
    w_relays(12, 8)
    phase("arrK")
    w_arrivals(9, 10, 11)
    phase("pairL")
    w_pairs(0, 1)
    phase("relL")
    w_relays(13, 14, 15)
    phase("o2")
    o_near(0)
    phase("pairM")
    w_pairs(3)
    phase("relM")
    w_relays(9, 10, 11)
    phase("o3")
    o_step(3)
    phase("pairN")
    w_pairs(4)
    phase("bundin")
    w_bundles_in()
    phase("pairO")
    w_last_early()
    phase("o3b")
    o_side(2)
    phase("pairP")
    w_last()
    phase("o4")
    o_near(1)
    o_near(3)
    phase("waitpair")
    got(wg.at[0:8], out_sem.at[2], r_wp.at[0], {"c": other})
    phase("waittok")
    got(tg.at[ym, 1], out_sem.at[6], r_t.at[2], {"y": ym})
    got(tg.at[yp, 0], out_sem.at[6], r_t.at[3], {"y": yp})
    got(tg.at[y2, 0], out_sem.at[6], r_t.at[4], {"y": ym})
    got(tg.at[y2, 1], out_sem.at[6], r_t.at[5], {"y": yp})
    o_left = list(range(4, len(o_plan)))

    def o_service(count=1):
        for _ in range(count):
            if o_left:
                o_step(o_left.pop(0))

    phase("proj")
    rows = 512
    ta = tg[:, 0].reshape(rows, 1024)
    tb = tg[:, 1].reshape(rows, 1024)

    def project(lo, hi):
        wa = wg[0:8, :, :, :, lo:hi].reshape(1024, hi - lo)
        wb = wg[8:16, :, :, :, lo:hi].reshape(1024, hi - lo)
        return jnp.dot(ta, wa, preferred_element_type=F32) + jnp.dot(tb, wb, preferred_element_type=F32)

    glu = (project(0, 256) * jax.nn.sigmoid(project(256, 512))).astype(BF16)
    glu_s[16 : 16 + rows] = glu
    for l in range(2):
        padf[l, 16:528] = glu[:, 128 * l : 128 * l + 128].astype(F32)
    send(glu_s.at[16:32], glu_s.at[528:544], out_sem.at[7], r_h.at[0], at_sp(prv))
    send(glu_s.at[512:528], glu_s.at[0:16], out_sem.at[7], r_h.at[1], at_sp(nxt))
    phase("service1")
    o_service()
    phase("projqkv")
    qkv = project(512, 896)
    kv_s[REACH : REACH + rows] = qkv[:, 256:].astype(BF16)
    q_s[...] = (qkv[:, :256] * 0.125).astype(BF16)
    send(kv_s.at[128:256], kv_s.at[640:768], out_sem.at[11], r_h.at[2], at_sp(prv))
    send(kv_s.at[512:640], kv_s.at[0:128], out_sem.at[11], r_h.at[3], at_sp(nxt))
    phase("service2")
    o_service()

    lane64 = lax.broadcasted_iota(jnp.int32, (64, 128), 1)

    def conv_rows(i, carry):
        r0 = i * 64
        accs = []
        for l in range(2):
            lanes = slice(128 * l, 128 * l + 128)
            acc = jnp.broadcast_to(cbias[0:1, lanes], (64, 128))
            for j in range(2 * HALF + 1):
                acc = acc + padf[l, pl.ds(r0 + j + 1, 64), :] * taps[j : j + 1, lanes]
            filt[pl.ds(r0, 64), lanes] = acc
            accs.append(acc)
        s1 = jnp.sum(accs[0] + accs[1], axis=1, keepdims=True)
        s2 = jnp.sum(accs[0] * accs[0] + accs[1] * accs[1], axis=1, keepdims=True)
        stat[pl.ds(r0, 64), :] = jnp.where(lane64 == 0, s1, jnp.where(lane64 == 1, s2, 0.0))
        return carry

    phase("conv")
    lax.fori_loop(1, 7, conv_rows, 0)
    phase("service3")
    o_service()
    phase("waithalo")
    got(glu_s.at[528:544], out_sem.at[7], r_h.at[0], at_sp(nxt))
    got(glu_s.at[0:16], out_sem.at[7], r_h.at[1], at_sp(prv))
    phase("conv2")
    first = (me > 0).astype(F32)
    last = (me < 127).astype(F32)
    for l in range(2):
        lanes = slice(128 * l, 128 * l + 128)
        padf[l, 0:16] = glu_s[0:16, lanes].astype(F32) * first
        padf[l, 528:544] = glu_s[528:544, lanes].astype(F32) * last
    conv_rows(0, 0)
    conv_rows(7, 0)
    st_tx[...] = jnp.transpose(stat[...])[0:8, :]

    phase("kvprep")
    low = lax.broadcasted_iota(jnp.int32, (512, 128), 1) < 64

    def widen(r0, n):
        kvf = kv_s[r0 : r0 + n].astype(F32)
        turned = pltpu.roll(kvf, 64, 1)
        lo = low[:n]
        kvw[0, r0 : r0 + n] = jnp.where(lo, kvf, 0.0).astype(BF16)
        kvw[1, r0 : r0 + n] = jnp.where(lo, 0.0, turned).astype(BF16)
        kvw[2, r0 : r0 + n] = jnp.where(lo, turned, 0.0).astype(BF16)
        kvw[3, r0 : r0 + n] = jnp.where(lo, 0.0, kvf).astype(BF16)

    widen(128, 512)
    for i, dev in enumerate((yp, ym, y2)):
        send(st_tx, st_rx.at[i], out_sem.at[8], r_st.at[0], {"y": dev})
    phase("waitkv")
    got(kv_s.at[640:768], out_sem.at[11], r_h.at[2], at_sp(nxt))
    got(kv_s.at[0:128], out_sem.at[11], r_h.at[3], at_sp(prv))
    phase("kvprep2")
    widen(0, 128)
    widen(640, 128)

    low128 = lax.broadcasted_iota(jnp.int32, (128, 128), 1) < 64
    ends = lax.broadcasted_iota(jnp.int32, (1, 384), 1)

    def attend(i):
        q0 = pl.multiple_of(i * 128, 128)
        pos = me * 512 + i * 128 - REACH + ends
        edge = jnp.where((pos >= 0) & (pos < 65536), 0.0, -1e30).astype(F32)
        bias = mask_s[...] + edge
        for p in range(2):
            qp = q_s[pl.ds(q0, 128), 128 * p : 128 * p + 128]
            probs, inverse = [], []
            for b in range(2):
                h = 2 * p + b
                s = nt_dot(qp, kvw[b, pl.ds(q0, 384), :]) + bias
                top = jnp.maximum(jnp.max(s, axis=1, keepdims=True), sink[h])
                e = jnp.exp(s - top)
                total = jnp.sum(e, axis=1, keepdims=True) + jnp.exp(sink[h] - top)
                lstat[pl.ds(q0, 128), h : h + 1] = top + jnp.log(total)
                probs.append(e.astype(BF16))
                inverse.append(1.0 / total)
            o = jnp.dot(probs[0], kvw[2, pl.ds(q0, 384), :], preferred_element_type=F32)
            o = o + jnp.dot(probs[1], kvw[3, pl.ds(q0, 384), :], preferred_element_type=F32)
            o = o * jnp.where(low128, inverse[0], inverse[1])
            feat[pl.ds(q0, 128), 256 + 128 * p : 384 + 128 * p] = o.astype(BF16)

    order = (y2, yp, ym, y)
    for n in range(3):
        phase(f"attend{n}")
        attend(order[n])
        if n == 1:
            phase("service4")
            o_service()
    phase("waitstat")
    got(st_rx, out_sem.at[8], r_st.at[0], {"y": ym})
    phase("norm")
    st_rx[0] = (st_tx[...] + st_rx[0] + st_rx[1] + st_rx[2]) * (1.0 / 1024.0)

    def norm_rows(i):
        r0 = pl.multiple_of(i * 128, 128)
        both = jnp.transpose(jnp.concatenate([st_rx[0, :, pl.ds(r0, 128)], jnp.zeros((120, 128), F32)], axis=0))
        mean = both[:, 0:1]
        var = both[:, 1:2] - mean * mean
        v = (filt[pl.ds(r0, 128), :] - mean) * lax.rsqrt(var + 1e-05) * ngain[...] + nbias[...]
        feat[pl.ds(r0, 128), 0:256] = (v * jax.nn.sigmoid(v)).astype(BF16)

    norm_rows(y2)

    def zcol(i, j):
        return lax.rem(z + 16 + 4 * i + (0, -1, 1, 2)[j], 16)

    ups = ([(0, 0), (0, 2)], [(1, 0)], [(3, 0), (3, 2)], [(2, 0)], [(0, 3), (1, 3)])
    downs = ([(0, 1)], [(1, 1), (1, 2)], [(3, 1)], [(2, 1), (2, 2)], [(2, 3), (3, 3)])
    u_at, d_at = (0, 2, 3, 5, 6, 8), (0, 1, 3, 4, 6, 8)

    def out_group(block, n):
        f = feat[pl.ds(pl.multiple_of(block * 128, 128), 128), :]
        w = jnp.concatenate([og[zcol(i, j)].reshape(128, 512) for i, j in ups[n] + downs[n]], axis=0)
        v = nt_dot(f, w)
        cut = [v[:, 128 * k : 128 * k + 128] for k in range(len(ups[n]) + len(downs[n]))]
        return cut[: len(ups[n])], cut[len(ups[n]) :]

    def put(ref, first, blocks):
        for k, v in enumerate(blocks):
            ref[first + k] = v.astype(ref.dtype)

    def columns_here(n):
        if n < 4:
            got(og.at[0:3, :, 0], out_sem.at[5], r_op.at[(0, 1, 3, 2)[n]], {"c": other})
        else:
            got(og.at[0:2], out_sem.at[5], r_op.at[4], {"c": other})

    def send_far(n):
        us, ds = pl.ds(u_at[n], len(ups[n])), pl.ds(d_at[n], len(downs[n]))
        send(tx2.at[0, us], rx2.at[0, us], out_sem.at[9], r_r2.at[n], {"y": yp})
        send(tx2.at[1, ds], rx2.at[1, ds], out_sem.at[9], r_r2.at[5 + n], {"y": ym})

    def far_group(n):
        phase(f"waitout{n}")
        columns_here(n)
        phase(f"far{n}")
        u, dn = out_group(y2, n)
        put(tx2.at[0], u_at[n], u)
        put(tx2.at[1], d_at[n], dn)

    far_group(0)
    far_group(1)
    send_far(0)
    far_group(2)
    send_far(1)
    norm_rows(yp)
    send_far(2)
    norm_rows(ym)
    phase("service7")
    o_service(len(o_left))
    far_group(3)
    far_group(4)
    send_far(3)
    phase("near")
    for n in range(5):
        u, dn = out_group(yp, n)
        put(part.at[0], u_at[n], u)
        put(tx4.at[0, 1], d_at[n], dn)
        if n == 0:
            send_far(4)
    for n in range(5):
        u, dn = out_group(ym, n)
        put(tx4.at[1, 0], u_at[n], u)
        put(part.at[1], d_at[n], dn)
        if n == 0:
            send(tx4.at[0, 1], rx4.at[0, 1], out_sem.at[10], r_rp.at[0], {"y": yp})
    phase("attendown")
    attend(y)
    send(tx4.at[1, 0], rx4.at[1, 0], out_sem.at[10], r_rp.at[1], {"y": ym})
    norm_rows(y)
    for n in range(5):
        u, dn = out_group(y, n)
        put(part.at[2], u_at[n], u)
        put(part.at[3], d_at[n], dn)

    def send_near(n):
        us, ds = pl.ds(u_at[n], len(ups[n])), pl.ds(d_at[n], len(downs[n]))
        send(tx4.at[0, 0, us], rx4.at[0, 0, us], out_sem.at[10], r_rp.at[2], {"y": yp})
        send(tx4.at[1, 1, ds], rx4.at[1, 1, ds], out_sem.at[10], r_rp.at[3], {"y": ym})

    phase("wait2")
    for n in range(5):
        us, ds = pl.ds(u_at[n], len(ups[n])), pl.ds(d_at[n], len(downs[n]))
        got(rx2.at[0, us], out_sem.at[9], r_r2.at[n], {"y": ym})
        tx4[0, 0, us] = (part[0, us] + rx2[0, us].astype(F32)).astype(BF16)
        got(rx2.at[1, ds], out_sem.at[9], r_r2.at[5 + n], {"y": yp})
        tx4[1, 1, ds] = (part[1, ds] + rx2[1, ds].astype(F32)).astype(BF16)
        if n:
            send_near(n - 1)
    phase("waitfin")
    log_out[...] = jnp.transpose(lstat[...])[0:4, :]
    send_near(4)
    got(rx4.at[0, 1], out_sem.at[10], r_rp.at[0], {"y": ym})
    got(rx4.at[1, 0], out_sem.at[10], r_rp.at[1], {"y": yp})
    got(rx4.at[0, 0], out_sem.at[10], r_rp.at[2], {"y": ym})
    got(rx4.at[1, 1], out_sem.at[10], r_rp.at[3], {"y": yp})
    phase("final")
    for way, at, sets in ((0, u_at, ups), (1, d_at, downs)):
        for n in range(5):
            for k, (i, j) in enumerate(sets[n]):
                p = at[n] + k
                total = part[2 + way, p] + rx4[0, way, p].astype(F32) + rx4[1, way, p].astype(F32)
                mixed[:, pl.ds(pl.multiple_of(zcol(i, j) * 128, 128), 128)] = total.astype(BF16)
    phase("drain")
    for i, ref in enumerate((
        wg.at[0:3], wg.at[0:13, 0:3, 0], wg.at[0:8], og.at[0:3, :, 0], og.at[0:6], og.at[0:8], tg.at[0:3],
        glu_s.at[0:32], st_rx, tx2, tx4, kv_s.at[0:256], og.at[0:3, 0, 0],
    )):
        copy(ref, ref, out_sem.at[i], r_wp.at[0], {"c": other}).wait_send()
    phase(None)


def on_device(
    tokens, in_gain, w_conv_val, w_conv_gate, w_query, w_key, value_weight, conv_taps, conv_bias,
    norm_gain, norm_bias, head_sink_logit, w_out_conv, w_out_attn,
):
    vm = pl.BlockSpec(memory_space=pltpu.VMEM)
    dma = pltpu.SemaphoreType.DMA
    scratch = [
        pltpu.VMEM((128, 2048), BF16),
        pltpu.VMEM((1, 2048), F32),
        pltpu.VMEM((16, 64), BF16),
        pltpu.VMEM((16, 64), BF16),
        pltpu.VMEM((31, 256), F32),
        pltpu.VMEM((1, 256), F32),
        pltpu.VMEM((1, 256), F32),
        pltpu.VMEM((1, 256), F32),
        pltpu.SMEM((4,), F32),
        pltpu.VMEM((16, 4, 2, 16, 896), BF16),
        pltpu.VMEM((16, 4, 2, 16, 512), BF16),
        pltpu.VMEM((4, 2, 128, 1024), BF16),
        pltpu.VMEM((544, 256), BF16),
        pltpu.VMEM((512, 256), BF16),
        pltpu.VMEM((768, 128), BF16),
        pltpu.VMEM((4, 768, 128), BF16),
        pltpu.VMEM((2, 544, 128), F32),
        pltpu.VMEM((512, 256), F32),
        pltpu.VMEM((512, 128), F32),
        pltpu.VMEM((512, 128), F32),
        pltpu.VMEM((8, 512), F32),
        pltpu.VMEM((3, 8, 512), F32),
        pltpu.VMEM((512, 512), BF16),
        pltpu.VMEM((128, 384), F32),
        pltpu.VMEM((4, 8, 128, 128), F32),
        pltpu.VMEM((2, 8, 128, 128), BF16),
        pltpu.VMEM((2, 8, 128, 128), BF16),
        pltpu.VMEM((2, 2, 8, 128, 128), BF16),
        pltpu.VMEM((2, 2, 8, 128, 128), BF16),
        dma((14,)),
    ]
    for n in (16, 16, 12, 1, 12, 4, 4, 5, 6, 4, 1, 10, 4, 13):
        scratch += [dma((n,))]
    mixed, log_total = pl.pallas_call(
        layer,
        name="layer",
        out_shape=(
            pltpu.VMEM((128, 2048), BF16),
            pltpu.VMEM((4, 512), F32),
        ),
        in_specs=[pl.BlockSpec(memory_space=pl.ANY)] * 14,
        out_specs=(vm, vm),
        scratch_shapes=scratch,
        compiler_params=pltpu.CompilerParams(
            collective_id=0, has_side_effects=True, vmem_limit_bytes=56 * 1024 * 1024
        ),
    )(
        tokens, in_gain[None], w_conv_val, w_conv_gate, w_query, w_key, value_weight,
        w_out_conv.T, w_out_attn.T, conv_taps, conv_bias[None], norm_gain[None], norm_bias[None],
        head_sink_logit,
    )
    return mixed, log_total.T


def solution(mesh):
    finer = Mesh(mesh.devices.reshape(16, 4, 2, mesh.shape["tp"]), ("z", "x", "c", "y"))
    in_specs = (
        P(SP_TP, None), P(),
        P(SP, "y"), P(SP, "y"), P(SP, "y"), P(SP, "y"), P(SP, "y"),
        P(None, "y"), P("y"), P("y"), P("y"), P("y"),
        P("y", SP), P("y", SP),
    )
    return jax.shard_map(
        on_device, mesh=finer, in_specs=in_specs, out_specs=(P(SP_TP, None), P(SP, "y")), check_vma=False
    )
```
